32 devices in a mesh: ep: 8 (over z, y), tp: 4 (over x, core).
Axes of the slice: x: 2, y: 2, z: 4, core: 2. Of those that a mesh axis runs over, the one named last changes fastest.
Arguments:
- state_probe_logits: bfloat16 [8192, 1024], P('ep', 'tp'), may hold values from -6 to 6
- retention_logits: bfloat16 [8192, 1024], P('ep', 'tp'), may hold values from -12 to 12
- state_source_entries: bfloat16 [8192, 1024], P('ep', 'tp'), may hold values from -6 to 6
- state_result_switch_logits: bfloat16 [8192, 1024], P('ep', 'tp'), may hold values from -6 to 6
- retention_bound_margin: float32 [1024], P('tp'), may hold values from 0 to 0.07
- extra_fading_amount: float32 [8192, 8], P('ep', 'tp'), may hold values from -0.7 to 0
- state_result_scale: float32 [1024], P('tp'), may hold values from 0.1 to 1.9
- state_result_matrix: bfloat16 [1024, 2048], P(None, 'tp'), may hold values from -0.1875 to 0.1875
- second_slice_tokens: bfloat16 [4096, 2048], P('ep'), may hold values from -6 to 6
- specialist_assignment: int32 [4096, 2], P('ep'), may hold values from 0 to 7, all different within a row; in each aligned block of 128 rows (0 to 127, 128 to 255, ...) at most 64 rows name the same one
- selected_specialist_share: float32 [4096, 2], P('ep'), may hold values from 0.1 to 1
- leading_scale_vector: float32 [2048], replicated, may hold values from 0.1 to 1.9
- trailing_scale_vector: float32 [2048], replicated, may hold values from 0.1 to 1.9
- specialist_switch_matrix: bfloat16 [8, 2048, 2048], P('ep', None, 'tp'), may hold values from -0.3125 to 0.3125
- specialist_widen_matrix: bfloat16 [8, 2048, 2048], P('ep', None, 'tp'), may hold values from -0.3125 to 0.3125
- specialist_contract_matrix: bfloat16 [8, 2048, 2048], P('ep', 'tp'), may hold values from -0.125 to 0.125
Outputs:
- mixer_out: bfloat16 [8192, 2048], P('ep', 'tp')
- moe_out: bfloat16 [4096, 2048], P(('ep', 'tp'))
The draws below stay inside these ranges and needn't reach their ends.
Inputs may be any that keep to these rules, and one draw needn't show every extreme that they name: `specialist_assignment`: each row names 2 different experts. In each aligned block of 128 rows no expert is named by more than 64 rows, a bound that some block reaches.
All inputs are finite; a program needn't handle non-finite values.
Results may differ from the reference program's by a relative error of at most 0.012.
Values may be sent and summed in bfloat16 or wider, within the bound.
A program may use at most 128 MiB of HBM per device.

```python
import math
import jax
import jax.numpy as jnp
import numpy as np
from jax import lax

D = 2048
HEAD = 128
STATE_GROUPS = 8
STATE_FEATURES = 1024
SPAN_STEPS = 64
FFE = 2048
EXPERTS = 8
TOP_K = 2
MIX_EP = 1024
TOK_DEV = 128
MIX_TOKENS = 8192
MOE_TOKENS = 4096
CAPQ = 64
N_TP = 4


def draw_retention_logits(key, part):
    noise_key, shift_key = jax.random.split(key)
    span_rows = max(MIX_EP // 4, 1)
    span_count = MIX_TOKENS // span_rows
    noise = jax.random.normal(noise_key, (MIX_TOKENS, STATE_FEATURES), jnp.float32)
    shifts = jax.random.uniform(shift_key, (span_count,), jnp.float32, -1.0, 1.5)
    return (noise + jnp.repeat(shifts, span_rows)[:, None]).astype(jnp.bfloat16)


def draw_retention_bound_margin(key, part):
    head_key, slow_key, fast_key = jax.random.split(key, 3)
    picked = jax.random.uniform(head_key, (STATE_GROUPS,), jnp.float32)
    slow_heads = picked < 0.5
    slow_channel = jnp.repeat(slow_heads, HEAD)
    lower = math.log(0.5 / MIX_TOKENS)
    upper = math.log(4.0 / MIX_TOKENS)
    slow_gap = jnp.exp(jax.random.uniform(slow_key, (STATE_FEATURES,), jnp.float32, lower, upper))
    fast_gap = jax.random.uniform(fast_key, (STATE_FEATURES,), jnp.float32, 0.03, 0.07)
    return jnp.where(slow_channel, slow_gap, fast_gap)


def draw_extra_fading_amount(key, part):
    where_key, depth_key = jax.random.split(key)
    struck = jax.random.uniform(where_key, (MIX_TOKENS, STATE_GROUPS), jnp.float32) < 6.0 / MIX_TOKENS
    depth = jnp.log(jax.random.uniform(depth_key, (MIX_TOKENS, STATE_GROUPS), jnp.float32, 0.5, 0.8))
    return jnp.where(struck, depth, jnp.zeros((), jnp.float32))


def block_levels(key, dims, pieces, smallest, largest):
    level = 1.0
    for position, shards_of in pieces:
        steps = jax.random.uniform(jax.random.fold_in(jax.random.fold_in(key, 6), position), (shards_of,), jnp.float32, smallest / len(pieces), largest / len(pieces))
        level = level * jnp.repeat(jnp.exp(steps), dims[position] // shards_of).reshape((-1,) + (1,) * (len(dims) - 1 - position))
    return level


def deal_out(key, own, number, rows, count, top, reach, lean):
    order = jax.random.permutation(key, count)
    packed, ordinary = shares(count, rows * top, reach, lean, True), shares(count, rows * top, reach, lean, False)
    places = jnp.arange(count)

    def named(tallies, rotation):
        used = int((tallies > 0).sum())
        fixed = max(1, used // 4)
        passed = fixed + (places - fixed + rotation * (used - fixed)) % max(1, count - fixed)
        return jnp.zeros((count,), jnp.int32).at[order[jnp.where(places < fixed, places, passed)]].set(jnp.asarray(tallies, jnp.int32))

    tallies = jnp.where(number % 4 == 0, named(packed, number // 4), named(ordinary, number - number // 4 - 1))
    mixed = jax.random.permutation(jax.random.fold_in(own, 3), count)
    giver, receiver = mixed[0:count // 2 * 2:2], mixed[1:count // 2 * 2:2]
    slack = jnp.minimum(tallies[giver] - 1, reach - tallies[receiver]) // 2
    slack = jnp.where((giver == order[0]) | (receiver == order[0]) | (tallies[receiver] == 0), 0, jnp.maximum(slack, 0))
    passed = jax.random.randint(jax.random.fold_in(own, 4), (count // 2,), 0, 1 << 20) % (slack + 1)
    tallies = tallies.at[giver].add(-passed).at[receiver].add(passed)
    labels = jnp.searchsorted(jnp.cumsum(tallies), jnp.arange(rows * top), side="right").astype(jnp.int32)
    grid = labels.reshape(top, rows).T
    grid = grid[jax.random.permutation(jax.random.fold_in(own, 1), rows)]
    rotation = jax.random.randint(jax.random.fold_in(own, 2), (rows, 1), 0, top)
    return jnp.take_along_axis(grid, (jnp.arange(top)[None, :] + rotation) % top, axis=1)


def shares(count, total, limit, lean, full):
    weights = [(1 << 20) // math.isqrt(standing ** lean) + 1 for standing in range(1, count + 1)]
    largest = limit if full else min(limit, max(-(-total // count), total * weights[0] // sum(weights)))
    least = 1 if total - largest >= count - 1 else 0
    counts, surplus = [largest] + [least] * (count - 1), total - largest - least * (count - 1)
    while surplus > 0:
        candidates = [i for i in range(1, count) if counts[i] < largest] or [i for i in range(1, count) if counts[i] < limit]
        mass, remaining = sum([weights[i] for i in candidates]), surplus
        for i in candidates:
            addition = min(limit - counts[i], max(1, remaining * weights[i] // mass), surplus)
            counts[i] = counts[i] + addition
            surplus = surplus - addition
    return np.array(counts)


def normal_values(stream_key, shape, scale, most, pieces=(), held_as=jnp.bfloat16):
    drawn = scale * jax.random.normal(stream_key, shape, jnp.float32)
    if pieces:
        drawn = drawn * block_levels(stream_key, shape, pieces, -0.22, 0.18)
    return jnp.clip(drawn, -most, most).astype(held_as)


def setup_inputs(seed: int = 0) -> dict:
    seeds = jax.random.split(jax.random.key(seed), 17)
    state_probe_logits = normal_values(seeds[0], (MIX_TOKENS, STATE_FEATURES), 1.0, 6.0, ((0, 8), (1, 4)))
    retention_logits = draw_retention_logits(jax.random.fold_in(seeds[16], 71), 0)
    state_source_entries = normal_values(seeds[2], (MIX_TOKENS, STATE_FEATURES), 1.0, 6.0, ((0, 8), (1, 4)))
    state_result_switch_logits = normal_values(seeds[3], (MIX_TOKENS, STATE_FEATURES), 1.0, 6.0, ((0, 8), (1, 4)))
    retention_bound_margin = draw_retention_bound_margin(jax.random.fold_in(seeds[16], 71), 0)
    extra_fading_amount = draw_extra_fading_amount(jax.random.fold_in(seeds[16], 71), 0)
    state_result_scale = jnp.clip(1.0 + 0.18 * jax.random.normal(seeds[6], (STATE_FEATURES,), jnp.float32), 0.1, 1.9)
    state_result_matrix = normal_values(seeds[7], (STATE_FEATURES, D), STATE_FEATURES ** -0.5, 0.1875, ((1, 4),))
    second_slice_tokens = normal_values(seeds[8], (MOE_TOKENS, D), 1.0, 6.0, ((0, 8),))
    specialist_assignment_keys = jax.random.split(jax.random.fold_in(seeds[9], 1), MOE_TOKENS // TOK_DEV)
    specialist_assignment_turns = jax.random.permutation(jax.random.fold_in(seeds[9], 3), MOE_TOKENS // TOK_DEV)
    specialist_assignment = jax.vmap(lambda own, number: deal_out(jax.random.fold_in(seeds[9], 2), own, number, TOK_DEV, EXPERTS, TOP_K, CAPQ, 1))(specialist_assignment_keys, specialist_assignment_turns).reshape((MOE_TOKENS, TOP_K))
    selected_specialist_share = jnp.clip(jnp.exp(math.log(1.0) - 2.3025851 * jax.random.uniform(seeds[10], (MOE_TOKENS, TOP_K), jnp.float32) ** block_levels(seeds[10], (MOE_TOKENS, TOP_K), ((0, 8),), -0.2, 0.2)), 0.1, 1.0)
    leading_scale_vector = jnp.clip(1.0 + 0.18 * jax.random.normal(seeds[11], (D,), jnp.float32), 0.1, 1.9)
    trailing_scale_vector = jnp.clip(1.0 + 0.18 * jax.random.normal(seeds[12], (D,), jnp.float32), 0.1, 1.9)
    specialist_switch_matrix = normal_values(seeds[13], (EXPERTS, D, FFE), (D // 6) ** -0.5, 0.3125, ((0, 8), (2, 4)))
    specialist_widen_matrix = normal_values(seeds[14], (EXPERTS, D, FFE), (D // 6) ** -0.5, 0.3125, ((0, 8), (2, 4)))
    specialist_contract_matrix = normal_values(seeds[15], (EXPERTS, FFE, D), FFE ** -0.5, 0.125, ((0, 8), (1, 4)))
    return dict(state_probe_logits=state_probe_logits, retention_logits=retention_logits, state_source_entries=state_source_entries, state_result_switch_logits=state_result_switch_logits, retention_bound_margin=retention_bound_margin, extra_fading_amount=extra_fading_amount, state_result_scale=state_result_scale, state_result_matrix=state_result_matrix, second_slice_tokens=second_slice_tokens, specialist_assignment=specialist_assignment, selected_specialist_share=selected_specialist_share, leading_scale_vector=leading_scale_vector, trailing_scale_vector=trailing_scale_vector, specialist_switch_matrix=specialist_switch_matrix, specialist_widen_matrix=specialist_widen_matrix, specialist_contract_matrix=specialist_contract_matrix)


NORM_EPS = 1e-06
SWISH_ALPHA = 1.702
CLAMP_LIMIT = 7.0
EXACT = lax.Precision.HIGHEST

def rms_scale(values, gain):
    return values * lax.rsqrt(lax.optimization_barrier(jnp.mean(values * values, axis=-1, keepdims=True)) + NORM_EPS) * gain

def clamped_unit(gate, upward):
    glued = jnp.minimum(gate, CLAMP_LIMIT)
    linear = jnp.clip(upward, -CLAMP_LIMIT, CLAMP_LIMIT)
    return glued * jax.nn.sigmoid(SWISH_ALPHA * glued) * (linear + 1.0)

def state_space_layer(state_probe_logits, retention_logits, state_source_entries, state_result_switch_logits, retention_bound_margin, extra_fading_amount, state_result_scale):
    total_rows = state_probe_logits.shape[0]
    span_tally = total_rows // SPAN_STEPS
    causal = jnp.tril(jnp.ones((SPAN_STEPS, SPAN_STEPS), jnp.float32))

    def per_head(values):
        return values.reshape(SPAN_STEPS, STATE_GROUPS, HEAD).transpose(1, 0, 2)

    def advance(state, operand_tensors):
        query_preact, forget_preact, value_preact, micro_batch_rows = operand_tensors
        query = per_head(jax.nn.silu(query_preact.astype(jnp.float32)) * HEAD ** (-0.5))
        input_key = per_head(retention_bound_margin * jax.nn.sigmoid(-forget_preact.astype(jnp.float32)))
        decay_logarithm = jnp.log1p(-input_key) + micro_batch_rows.T[:, :, None]
        values = per_head(value_preact.astype(jnp.float32))
        cumul = jnp.cumsum(decay_logarithm, axis=1)
        middle = cumul[:, SPAN_STEPS // 2 - 1:SPAN_STEPS // 2]
        last = cumul[:, SPAN_STEPS - 1:]
        scores = jnp.einsum('hid,hjd->hij', query * jnp.exp(cumul - middle), input_key * jnp.exp(middle - cumul), precision=EXACT) * causal
        inner = jnp.einsum('hij,hje->hie', scores, values, precision=EXACT)
        outer = jnp.einsum('hid,hde->hie', query * jnp.exp(cumul), state, precision=EXACT)
        update = jnp.einsum('hcd,hce->hde', input_key * jnp.exp(last - cumul), values, precision=EXACT)
        state = jnp.exp(last[:, 0])[:, :, None] * state + update
        return (state, inner + outer)
    operand_tensors = (state_probe_logits.reshape(span_tally, SPAN_STEPS, STATE_FEATURES), retention_logits.reshape(span_tally, SPAN_STEPS, STATE_FEATURES), state_source_entries.reshape(span_tally, SPAN_STEPS, STATE_FEATURES), extra_fading_amount.reshape(span_tally, SPAN_STEPS, STATE_GROUPS))
    final_state, raw_out = lax.scan(advance, jnp.zeros((STATE_GROUPS, HEAD, HEAD), jnp.float32), operand_tensors)
    normed = raw_out * lax.rsqrt(lax.optimization_barrier(jnp.mean(raw_out * raw_out, axis=-1, keepdims=True)) + NORM_EPS)
    normed = normed.transpose(0, 2, 1, 3).reshape(total_rows, STATE_FEATURES)
    return (normed * state_result_scale * jax.nn.silu(state_result_switch_logits.astype(jnp.float32))).astype(jnp.bfloat16)

def experts(second_slice_tokens, specialist_assignment, selected_specialist_share, leading_scale_vector, trailing_scale_vector, specialist_switch_matrix, specialist_widen_matrix, specialist_contract_matrix):
    token_count = second_slice_tokens.shape[0]
    span_tally = token_count // TOK_DEV
    normed = rms_scale(second_slice_tokens.astype(jnp.float32), leading_scale_vector).astype(jnp.bfloat16)
    per_block = TOK_DEV * TOP_K
    flat = specialist_assignment.reshape(span_tally, per_block)
    onehot = (flat[:, :, None] == jnp.arange(EXPERTS, dtype=jnp.int32)[None, None, :]).astype(jnp.int32)
    rank = lax.optimization_barrier(jnp.sum(onehot * (jnp.cumsum(onehot, axis=1) - 1), axis=2))
    slots = ((flat * span_tally + jnp.arange(span_tally, dtype=jnp.int32)[:, None]) * CAPQ + rank).reshape(-1)
    owner = jnp.arange(token_count * TOP_K, dtype=jnp.int32) // TOP_K
    per_expert = span_tally * CAPQ
    room = EXPERTS * per_expert
    source = jnp.zeros((room,), jnp.int32).at[slots].set(owner)
    filled = jnp.zeros((room,), jnp.int32).at[slots].set(1)
    width = FFE // N_TP

    def one_expert(operand_tensors):
        rows_source, rows_live, gate_w, up_w, down_w = operand_tensors
        chosen = jnp.where(rows_live[:, None] > 0, normed[rows_source], jnp.zeros((), jnp.bfloat16))
        gate = jnp.dot(chosen, gate_w, preferred_element_type=jnp.float32)
        upward = jnp.dot(chosen, up_w, preferred_element_type=jnp.float32)
        activated = clamped_unit(gate, upward).astype(jnp.bfloat16)
        parts = jnp.einsum('rjf,jfd->jrd', activated.reshape(per_expert, N_TP, width).astype(jnp.float32), down_w.reshape(N_TP, width, D).astype(jnp.float32))
        parts = lax.optimization_barrier(parts.astype(jnp.bfloat16))
        return lax.optimization_barrier(jnp.sum(parts.astype(jnp.float32), axis=0)).astype(jnp.bfloat16)
    outputs = lax.map(one_expert, (source.reshape(EXPERTS, per_expert), filled.reshape(EXPERTS, per_expert), specialist_switch_matrix, specialist_widen_matrix, specialist_contract_matrix))
    flat_out = outputs.reshape(room, D)
    token_slots = slots.reshape(token_count, TOP_K)
    combined = jnp.zeros((token_count, D), jnp.float32)
    for column in range(TOP_K):
        combined = combined + flat_out[token_slots[:, column]].astype(jnp.float32) * selected_specialist_share[:, column:column + 1]
    return rms_scale(combined, trailing_scale_vector).astype(jnp.bfloat16)

def reference(state_probe_logits, retention_logits, state_source_entries, state_result_switch_logits, retention_bound_margin, extra_fading_amount, state_result_scale, state_result_matrix, second_slice_tokens, specialist_assignment, selected_specialist_share, leading_scale_vector, trailing_scale_vector, specialist_switch_matrix, specialist_widen_matrix, specialist_contract_matrix):
    state_layer_result = state_space_layer(state_probe_logits, retention_logits, state_source_entries, state_result_switch_logits, retention_bound_margin, extra_fading_amount, state_result_scale)
    mixer_out = jnp.dot(state_layer_result, state_result_matrix, preferred_element_type=jnp.float32).astype(jnp.bfloat16)
    moe_out = experts(second_slice_tokens, specialist_assignment, selected_specialist_share, leading_scale_vector, trailing_scale_vector, specialist_switch_matrix, specialist_widen_matrix, specialist_contract_matrix)
    return (mixer_out, moe_out)
```

```python
import functools

import jax
import jax.numpy as jnp
from jax import lax
from jax.experimental import pallas as pl
from jax.experimental.pallas import tpu as pltpu
from jax.sharding import PartitionSpec as P

HEAD = 128
SPAN = 128
TOK_DEV = 128
STAGES = 4
PIECES = 4
STEP = 512
TILE = 16

NORM_EPS = 1e-06
SWISH_ALPHA = 1.702
CLAMP_LIMIT = 7.0
MESH = pl.DeviceIdType.MESH
VMEM = pltpu.VMEM
DMA = pltpu.SemaphoreType.DMA
NT = (((1,), (1,)), ((), ()))
TN = (((0,), (0,)), ((), ()))


def remote(src, dst, send, recv, where):
    return pltpu.make_async_remote_copy(
        src_ref=src, dst_ref=dst, send_sem=send, recv_sem=recv, device_id=where, device_id_type=MESH
    )


def clamped_unit(gate, upward):
    glued = jnp.minimum(gate, CLAMP_LIMIT)
    linear = jnp.clip(upward, -CLAMP_LIMIT, CLAMP_LIMIT)
    return glued * jax.nn.sigmoid(SWISH_ALPHA * glued) * (linear + 1.0)


def rms_scale(values, gain):
    return values * lax.rsqrt(jnp.mean(values * values, axis=-1, keepdims=True) + NORM_EPS) * gain


def span_step(t, probe, ret, val, margin, extra, raw, qdec, state, running):
    rows = pl.ds(pl.multiple_of(t * SPAN, SPAN), SPAN)
    width = probe.shape[1]
    x = probe[rows, :].astype(jnp.float32)
    q = x * jax.nn.sigmoid(x) * HEAD ** (-0.5)
    k = margin[...] * jax.nn.sigmoid(-ret[rows, :].astype(jnp.float32))
    logs = jnp.log1p(-k)
    row = lax.broadcasted_iota(jnp.int32, (SPAN, SPAN), 0)
    col = lax.broadcasted_iota(jnp.int32, (SPAN, SPAN), 1)
    causal = row >= col
    tril = jnp.where(causal, 1.0, 0.0).astype(jnp.float32)
    for h in range(width // HEAD):
        cols = slice(h * HEAD, (h + 1) * HEAD)
        qh, kh = q[:, cols], k[:, cols]
        fade = jnp.transpose(jnp.broadcast_to(extra[h : h + 1, rows], (SPAN, SPAN)))
        ld = logs[:, cols] + fade
        cum = jnp.dot(
            tril, ld, precision=lax.Precision.HIGHEST, preferred_element_type=jnp.float32
        )
        middle = cum[SPAN // 2 - 1 : SPAN // 2, :]
        last = cum[SPAN - 1 :, :]
        a = (qh * jnp.exp(cum - middle)).astype(jnp.bfloat16)
        b = (kh * jnp.exp(middle - cum)).astype(jnp.bfloat16)
        qe = qh * jnp.exp(cum)
        kd = (kh * jnp.exp(last - cum)).astype(jnp.bfloat16)
        v = val[rows, cols]
        s = lax.dot_general(a, b, NT, preferred_element_type=jnp.float32)
        s = jnp.where(causal, s, 0.0).astype(jnp.bfloat16)
        st = state[h]
        out = jnp.dot(s, v, preferred_element_type=jnp.float32)
        out = out + lax.dot_general(
            qe.astype(jnp.bfloat16), st.astype(jnp.bfloat16), NT, preferred_element_type=jnp.float32
        )
        raw[rows, cols] = out
        before = running[0:1, cols]
        qdec[rows, cols] = (qe * jnp.exp(before)).astype(jnp.bfloat16)
        state[h] = jnp.exp(last) * st + lax.dot_general(
            v, kd, TN, preferred_element_type=jnp.float32
        )
        running[:, cols] = running[:, cols] + last


def kernel(
    n, planes, capacity, experts, table, margin, extra, scale, lead, trail,
    tok_hbm, probe_hbm, ret_hbm, val_hbm, switch_hbm, mix_hbm, gate_hbm, up_hbm, down_hbm,
    mix_out, moe_out,
    nt, probe, ret, val, switch, mix_w, gate_w, up_w, down_w,
    rk, sh, meta, relay, rows, part, acc, sendb, recvb, fin, back, pk, pko, comb, spread,
    raw, qdec, state, state_bf, running, plst, pld, chain_in, chain_out, enter, carry, gath,
    load_sem,
    fsend, frecv, msend, mrecv, ysend, yrecv, zsend, zrecv,
    xsend, xrecv, csend, crecv, dsend, drecv,
    esend0, erecv0, esend1, erecv1, bsend, brecv, rsend, rrecv,
    pssend, psrecv, pdsend, pdrecv, chsend, chrecv,
    gxsend, gxrecv, gcsend, gcrecv, gdsend, gdrecv,
):
    i, j = lax.axis_index("ep"), lax.axis_index("tp")
    mate = j + 1 - 2 * (j % 2)
    cross = (j + 2) % 4
    mate_cross = (mate + 2) % 4
    group = n // planes
    p, g = i // group, i % group
    features = nt.shape[2]
    heads = state.shape[0]
    width = probe.shape[1]
    length = probe.shape[0]
    f32, bf = jnp.float32, jnp.bfloat16

    pairs = (
        (tok_hbm, nt), (probe_hbm, probe), (ret_hbm, ret), (val_hbm, val),
        (gate_hbm, gate_w), (up_hbm, up_w), (down_hbm, down_w),
        (switch_hbm, switch), (mix_hbm, mix_w),
    )
    loads = [pltpu.make_async_copy(a, b, load_sem.at[w]) for w, (a, b) in enumerate(pairs)]
    for load in loads:
        load.start()

    barrier = pltpu.get_barrier_semaphore()

    def hello(s, c):
        pl.semaphore_signal(barrier, inc=1, device_id=((i + s) % n, j), device_id_type=MESH)
        return c

    lax.fori_loop(1, n, hello, 0)
    for t in (mate, cross):
        pl.semaphore_signal(barrier, inc=1, device_id=(i, t), device_id_type=MESH)

    def plane(s):
        left, right = p, planes - 1 - p
        big = (left - right + planes) // planes
        small = big * right + (1 - big) * left
        t = s - 1 + 2 * planes
        both = 1 - (t - 2 * small) // (2 * planes)
        t = t - 2 * planes
        far = both * ((t + 2) // 2) + (1 - both) * (s - small)
        sign = (2 * big - 1) * (2 * both * (s % 2) - 1)
        other = (s + planes - 1) // planes - s // planes
        return p + other * sign * far

    def place(c):
        s = (c + 1) // group
        q = plane(s)
        return s, q, q * group + (g + (c + 1) % group) % group

    def ranks():
        ids = lax.broadcasted_iota(jnp.int32, (experts, TOK_DEV), 0).astype(f32)
        one = lax.broadcasted_iota(jnp.int32, (TOK_DEV, TOK_DEV), 0)
        two = lax.broadcasted_iota(jnp.int32, (TOK_DEV, TOK_DEV), 1)
        earlier = jnp.where(one < two, 1.0, 0.0).astype(bf)
        top = table.shape[0] // 2
        for b in range(4):
            lanes = slice(b * TOK_DEV, (b + 1) * TOK_DEV)
            named = jnp.zeros((experts, TOK_DEV), f32)
            share = jnp.zeros((experts, TOK_DEV), f32)
            for w in range(top):
                hit = ids == table[w : w + 1, lanes]
                named = named + jnp.where(hit, 1.0, 0.0)
                share = share + jnp.where(hit, table[top + w : top + w + 1, lanes], 0.0)
            ahead = jnp.dot(named.astype(bf), earlier, preferred_element_type=f32)
            rk[b] = jnp.where(named > 0.5, ahead, -1.0)
            sh[b] = share

    def norm(b):
        def tile(t, c):
            r = pl.ds(pl.multiple_of(t * TILE, TILE), TILE)
            nt[b, r, :] = rms_scale(nt[b, r, :].astype(f32), lead[...]).astype(bf)
            return c

        lax.fori_loop(0, TOK_DEV // TILE, tile, 0)

    slot = lax.broadcasted_iota(jnp.int32, (capacity, TOK_DEV), 0).astype(f32)

    def one_hot(ranked, e):
        return jnp.where(slot == ranked[pl.ds(e, 1), :], 1.0, 0.0)

    def pack(ranked, tokens, own, others):
        picks = [one_hot(ranked, i)]
        if others is not None:
            picks += [one_hot(ranked, p * group + (g + r) % group) for r in range(1, group)]
        pick = (picks[0] if len(picks) == 1 else jnp.concatenate(picks, axis=0)).astype(bf)
        for f in range(0, features, STEP):
            y = jnp.dot(pick, tokens[:, f : f + STEP], preferred_element_type=f32).astype(bf)
            own[:, f : f + STEP] = y[:capacity]
            for r in range(1, len(picks)):
                others[r - 1, :, f : f + STEP] = y[r * capacity : (r + 1) * capacity]

    def step_right(q, src, info):
        return (
            remote(src, relay.at[q], fsend.at[0, q], frecv.at[q], (i + group, j)),
            remote(info, meta.at[q], msend.at[0, q], mrecv.at[q], (i + group, j)),
        )

    def step_left(q, src, info):
        return (
            remote(src, relay.at[q], fsend.at[1, q], frecv.at[q], (i - group, j)),
            remote(info, meta.at[q], msend.at[1, q], mrecv.at[q], (i - group, j)),
        )

    def over_y(q, r):
        k = q * group + g
        d = p * group + (g + r) % group
        return remote(pk.at[q, r - 1], rows.at[k, j], ysend.at[q, r], yrecv.at[k], (d, j))

    def got_y(k):
        return remote(pk.at[0, 0], rows.at[k, j], ysend.at[0, 0], yrecv.at[k], (i, mate))

    def near(r, w):
        d = p * group + (g + r) % group
        b = (j, cross)[w]
        return remote(pko.at[w, r - 1], rows.at[i, b], zsend.at[w, r], zrecv.at[w, i], (d, j))

    def got_near(k, w):
        b = (j, cross)[w]
        return remote(pko.at[w, 0], rows.at[k, b], zsend.at[w, 0], zrecv.at[w, k], (i, mate))

    def over_x(k):
        return remote(rows.at[k, j], rows.at[k, j], xsend.at[k], xrecv.at[k], (i, cross))

    def over_c(k):
        return remote(rows.at[k, j], rows.at[k, j], csend.at[k], crecv.at[k], (i, mate))

    def over_d(k):
        return remote(rows.at[k, cross], rows.at[k, cross], dsend.at[k], drecv.at[k], (i, mate))

    def to_mate(k, close):
        if close:
            return remote(part.at[k, mate], acc.at[0, k], esend0.at[k], erecv0.at[k], (i, mate))
        return remote(
            part.at[k, mate_cross], acc.at[1, k], esend1.at[k], erecv1.at[k], (i, mate)
        )

    def to_cross(k):
        return remote(sendb.at[k], recvb.at[k], bsend.at[k], brecv.at[k], (i, cross))

    def home(k):
        return remote(fin.at[k], back.at[i], rsend.at[k], rrecv.at[i], (k, j))

    def home_in(k):
        return remote(fin.at[k], back.at[k], rsend.at[k], rrecv.at[k], (k, j))

    def arrive(s):
        q = plane(s)
        k = q * group + g
        for copy in step_right(q, relay.at[q], meta.at[q]):
            copy.wait_recv()

        @pl.when((q < p) & (p + 1 < planes))
        def _():
            for copy in step_right(q, relay.at[q], meta.at[q]):
                copy.start()

        @pl.when((q > p) & (p >= 1))
        def _():
            for copy in step_left(q, relay.at[q], meta.at[q]):
                copy.start()

        pack(meta.at[q], relay.at[q], rows.at[k, j], pk.at[q])
        over_x(k).start()
        over_c(k).start()
        for r in range(1, group):
            over_y(q, r).start()

    def arrive_y(s):
        q = plane(s)
        for r in range(1, group):
            k = q * group + (g + r) % group
            got_y(k).wait_recv()
            over_x(k).start()
            over_c(k).start()

    def work(c):
        s, q, k = place(c)

        @pl.when((s >= 1) & (s < planes))
        def _():
            over_x(k).wait_recv()
            over_d(k).start()

        @pl.when(s < planes)
        def _():
            over_c(k).wait_recv()
            over_d(k).wait_recv()

        x = rows[k].reshape(4 * capacity, features)
        gate = jnp.dot(x, gate_w[...], preferred_element_type=f32)
        upward = jnp.dot(x, up_w[...], preferred_element_type=f32)
        act = clamped_unit(gate, upward).astype(bf)
        for f in range(0, features, STEP):
            y = jnp.dot(act, down_w[:, f : f + STEP], preferred_element_type=f32)
            part[k, :, :, f : f + STEP] = y.astype(bf).reshape(4, capacity, STEP)
        to_mate(k, False).start()
        to_mate(k, True).start()

    def first_sum(c):
        s, q, k = place(c)
        to_mate(k, False).wait()
        x = part[k, cross].astype(f32) + acc[1, k].astype(f32)
        sendb[k] = x.astype(bf)
        to_cross(k).start()

    def total(c):
        s, q, k = place(c)
        to_mate(k, True).wait()
        to_cross(k).wait()
        x = part[k, j].astype(f32) + acc[0, k].astype(f32)
        fin[k] = (x + recvb[k].astype(f32)).astype(bf)

        @pl.when(s < planes)
        def _():
            home(k).start()

    def in_plane(r):
        d = p * group + (g + r) % group
        return (
            remote(state_bf, plst.at[g], pssend.at[r], psrecv.at[g], (d, j)),
            remote(running, pld.at[g], pdsend.at[r], pdrecv.at[g], (d, j)),
        )

    def in_plane_got(r):
        o = (g + r) % group
        return (
            remote(state_bf, plst.at[o], pssend.at[r], psrecv.at[o], (i, mate)),
            remote(running, pld.at[o], pdsend.at[r], pdrecv.at[o], (i, mate)),
        )

    def chain():
        return remote(chain_out, chain_in, chsend, chrecv, (i + group, j))

    def prefix():
        for r in range(1, group):
            for copy in in_plane_got(r):
                copy.wait_recv()

        @pl.when(p == 0)
        def _():
            carry[...] = jnp.zeros_like(carry)

        @pl.when(p >= 1)
        def _():
            chain().wait_recv()
            carry[...] = chain_in[...].astype(f32)

        for o in range(group):
            @pl.when(g == o)
            def _():
                enter[...] = carry[...]

            for h in range(heads):
                d = pld[o, 0:1, h * HEAD : (h + 1) * HEAD]
                carry[h] = jnp.exp(d) * carry[h] + plst[o, h].astype(f32)

        @pl.when(p + 1 < planes)
        def _():
            chain_out[...] = carry[...].astype(bf)
            chain().start()

    piece = length // PIECES

    def at(c):
        return pl.ds(pl.multiple_of(c * piece, piece), piece)

    def mix_x(c):
        here = gath.at[j, at(c)]
        return remote(here, here, gxsend.at[c], gxrecv.at[c], (i, cross))

    def mix_c(c):
        here = gath.at[j, at(c)]
        return remote(here, here, gcsend.at[c], gcrecv.at[c], (i, mate))

    def mix_d(c):
        here = gath.at[cross, at(c)]
        return remote(here, here, gdsend.at[c], gdrecv.at[c], (i, mate))

    def mix_final(c, z):
        r = at(c)
        for h in range(heads):
            cols = slice(h * HEAD, (h + 1) * HEAD)
            x = raw[r, cols] + lax.dot_general(
                qdec[r, cols], enter[h].astype(bf), NT, preferred_element_type=f32
            )
            x = x * lax.rsqrt(jnp.mean(x * x, axis=-1, keepdims=True) + NORM_EPS)
            v = switch[r, cols].astype(f32)
            gath[j, r, cols] = (x * scale[:, cols] * (v * jax.nn.sigmoid(v))).astype(bf)
        mix_x(c).start()
        mix_c(c).start()
        return z

    def mix_pass(c, z):
        mix_x(c).wait()
        mix_d(c).start()
        return z

    def mix_project(c, z):
        mix_c(c).wait()
        mix_d(c).wait()
        r = at(c)
        a = jnp.dot(gath[0, r, :], mix_w[0:width, :], preferred_element_type=f32)
        for w in range(1, 4):
            a = a + jnp.dot(
                gath[w, r, :], mix_w[w * width : (w + 1) * width, :], preferred_element_type=f32
            )
        mix_out[r, :] = a.astype(bf)
        return z

    ranks()
    loads[0].wait()
    norm(j)
    pl.semaphore_wait(barrier, n + 1)

    @pl.when(p + 1 < planes)
    def _():
        for copy in step_right(p, nt.at[j], rk.at[j]):
            copy.start()

    @pl.when(p >= 1)
    def _():
        for copy in step_left(p, nt.at[j], rk.at[j]):
            copy.start()

    norm(cross)
    for w, b in enumerate((j, cross)):
        pack(rk.at[b], nt.at[b], rows.at[i, b], pko.at[w])
        for r in range(1, group):
            near(r, w).start()
    norm(mate)
    norm(mate_cross)
    for b in (mate, mate_cross):
        pack(rk.at[b], nt.at[b], rows.at[i, b], None)

    for load in loads[1:4]:
        load.wait()
    state[...] = jnp.zeros_like(state)
    running[...] = jnp.zeros_like(running)

    def spans(t, c):
        span_step(t, probe, ret, val, margin, extra, raw, qdec, state, running)
        return c

    lax.fori_loop(0, length // SPAN, spans, 0)
    for h in range(heads):
        state_bf[h] = state[h].astype(bf)
    plst[g] = state_bf[...]
    pld[g] = running[...]
    for r in range(1, group):
        for copy in in_plane(r):
            copy.start()
    for r in range(1, group):
        k = p * group + (g + r) % group
        got_near(k, 0).wait_recv()
        over_c(k).start()
        got_near(k, 1).wait_recv()
        over_d(k).start()
    for load in loads[4:]:
        load.wait()

    def pump(u, z):
        @pl.when(u < planes - 1)
        def _():
            arrive(u + 1)

        @pl.when(u < n)
        def _():
            work(u)

        @pl.when((u >= 1) & (u < n + 1))
        def _():
            first_sum(u - 1)

        @pl.when((u >= 2) & (u < n + 2))
        def _():
            total(u - 2)

        @pl.when(u == 0)
        def _():
            prefix()

        @pl.when(u < planes - 1)
        def _():
            arrive_y(u + 1)

        @pl.when(u == planes - 1)
        def _():
            lax.fori_loop(0, PIECES, mix_final, 0)

        @pl.when(u == planes)
        def _():
            lax.fori_loop(0, PIECES, mix_pass, 0)

        @pl.when(u == planes + 1)
        def _():
            lax.fori_loop(0, PIECES, mix_project, 0)

        return z

    lax.fori_loop(0, n + 2, pump, 0)
    back[i] = fin[i]

    def weigh(e, z):
        r = pl.ds(pl.multiple_of(e * capacity, capacity), capacity)
        spread[r, :] = jnp.where(
            slot == rk[j, pl.ds(e, 1), :], jnp.broadcast_to(sh[j, pl.ds(e, 1), :], slot.shape), 0.0
        )
        return z

    lax.fori_loop(0, experts, weigh, 0)
    wide = spread[...]
    high = wide.astype(bf)
    low = (wide - high.astype(f32)).astype(bf)

    def collect(s, z):
        k = (i + s) % n
        home_in(k).wait_recv()
        return z

    lax.fori_loop(1, n, collect, 0)
    for f in range(0, features, STEP):
        flat = back[:, :, f : f + STEP].reshape(n * capacity, STEP)
        comb[:, f : f + STEP] = lax.dot_general(
            high, flat, TN, preferred_element_type=f32
        ) + lax.dot_general(low, flat, TN, preferred_element_type=f32)

    def closing(t, z):
        r = pl.ds(pl.multiple_of(t * TILE, TILE), TILE)
        moe_out[r, :] = rms_scale(comb[r, :], trail[...]).astype(bf)
        return z

    lax.fori_loop(0, TOK_DEV // TILE, closing, 0)

    def finish(s, z):
        k = (i + s) % n
        over_c(k).wait_send()
        over_d(k).wait_send()
        home(k).wait_send()
        return z

    lax.fori_loop(1, n, finish, 0)

    def finish_far(s, z):
        q = plane(s)
        for r in range(group):
            over_x(q * group + r).wait_send()
        for r in range(1, group):
            over_y(q, r).wait_send()

        @pl.when((q < p) & (p + 1 < planes))
        def _():
            for copy in step_right(q, relay.at[q], meta.at[q]):
                copy.wait_send()

        @pl.when((q > p) & (p >= 1))
        def _():
            for copy in step_left(q, relay.at[q], meta.at[q]):
                copy.wait_send()

        return z

    lax.fori_loop(1, planes, finish_far, 0)

    @pl.when(p + 1 < planes)
    def _():
        for copy in step_right(p, nt.at[j], rk.at[j]):
            copy.wait_send()
        chain().wait_send()

    @pl.when(p >= 1)
    def _():
        for copy in step_left(p, nt.at[j], rk.at[j]):
            copy.wait_send()

    for r in range(1, group):
        for w in range(2):
            near(r, w).wait_send()
        for copy in in_plane(r):
            copy.wait_send()


def shards(
    state_probe_logits,
    retention_logits,
    state_source_entries,
    state_result_switch_logits,
    retention_bound_margin,
    extra_fading_amount,
    state_result_scale,
    state_result_matrix,
    second_slice_tokens,
    specialist_assignment,
    selected_specialist_share,
    leading_scale_vector,
    trailing_scale_vector,
    specialist_switch_matrix,
    specialist_widen_matrix,
    specialist_contract_matrix,
):
    n = lax.axis_size("ep")
    experts = specialist_switch_matrix.shape[0] * n
    top_count = specialist_assignment.shape[1]
    capacity = 2 * TOK_DEV * top_count // experts
    planes = max(d for d in range(1, STAGES + 1) if n % d == 0)
    group = n // planes
    length, width = state_probe_logits.shape
    heads = width // HEAD
    features = second_slice_tokens.shape[1]
    hidden = specialist_switch_matrix.shape[2]
    columns = state_result_matrix.shape[1]
    bf, f32 = jnp.bfloat16, jnp.float32
    table = jnp.concatenate(
        [specialist_assignment.astype(f32), selected_specialist_share], axis=1
    ).T
    vm = pl.BlockSpec(memory_space=VMEM)
    hbm = pl.BlockSpec(memory_space=pl.ANY)
    chunk = (capacity, features)
    block = (TOK_DEV, features)
    return tuple(
        pl.pallas_call(
            functools.partial(kernel, n, planes, capacity, experts),
            name="fused",
            out_shape=(
                jax.ShapeDtypeStruct((length, columns), bf),
                jax.ShapeDtypeStruct(block, bf),
            ),
            in_specs=[vm] * 6 + [hbm] * 9,
            out_specs=(vm, vm),
            scratch_shapes=[
                VMEM((4,) + block, bf),
                VMEM((length, width), bf),
                VMEM((length, width), bf),
                VMEM((length, width), bf),
                VMEM((length, width), bf),
                VMEM(state_result_matrix.shape, bf),
                VMEM((features, hidden), bf),
                VMEM((features, hidden), bf),
                VMEM((hidden, features), bf),
                VMEM((4, experts, TOK_DEV), f32),
                VMEM((4, experts, TOK_DEV), f32),
                VMEM((planes, experts, TOK_DEV), f32),
                VMEM((planes,) + block, bf),
                VMEM((n, 4) + chunk, bf),
                VMEM((n, 4) + chunk, bf),
                VMEM((2, n) + chunk, bf),
                VMEM((n,) + chunk, bf),
                VMEM((n,) + chunk, bf),
                VMEM((n,) + chunk, bf),
                VMEM((n,) + chunk, bf),
                VMEM((planes, group - 1) + chunk, bf),
                VMEM((2, group - 1) + chunk, bf),
                VMEM(block, f32),
                VMEM((n * capacity, TOK_DEV), f32),
                VMEM((length, width), f32),
                VMEM((length, width), bf),
                VMEM((heads, HEAD, HEAD), f32),
                VMEM((heads, HEAD, HEAD), bf),
                VMEM((8, width), f32),
                VMEM((group, heads, HEAD, HEAD), bf),
                VMEM((group, 8, width), f32),
                VMEM((heads, HEAD, HEAD), bf),
                VMEM((heads, HEAD, HEAD), bf),
                VMEM((heads, HEAD, HEAD), f32),
                VMEM((heads, HEAD, HEAD), f32),
                VMEM((4, length, width), bf),
                DMA((9,)),
                DMA((2, planes)), DMA((planes,)), DMA((2, planes)), DMA((planes,)),
                DMA((planes, group)), DMA((n,)), DMA((2, group)), DMA((2, n)),
            ]
            + [DMA((n,))] * 14
            + [DMA((group,))] * 4
            + [DMA, DMA]
            + [DMA((PIECES,))] * 6,
            compiler_params=pltpu.CompilerParams(
                collective_id=0, has_side_effects=True, vmem_limit_bytes=62 * 2**20
            ),
        )(
            table,
            retention_bound_margin[None, :],
            extra_fading_amount.T,
            state_result_scale[None, :],
            leading_scale_vector[None, :],
            trailing_scale_vector[None, :],
            second_slice_tokens.reshape((4,) + block),
            state_probe_logits,
            retention_logits,
            state_source_entries,
            state_result_switch_logits,
            state_result_matrix,
            specialist_switch_matrix[0],
            specialist_widen_matrix[0],
            specialist_contract_matrix[0],
        )
    )


def solution(mesh):
    return jax.shard_map(
        shards,
        mesh=mesh,
        in_specs=(
            P("ep", "tp"),
            P("ep", "tp"),
            P("ep", "tp"),
            P("ep", "tp"),
            P("tp"),
            P("ep", "tp"),
            P("tp"),
            P(None, "tp"),
            P("ep", None),
            P("ep", None),
            P("ep", None),
            P(),
            P(),
            P("ep", None, "tp"),
            P("ep", None, "tp"),
            P("ep", "tp", None),
        ),
        out_specs=(P("ep", "tp"), P(("ep", "tp"), None)),
        check_vma=False,
    )
```

```python
import functools

import jax
import jax.numpy as jnp
from jax import lax
from jax.experimental import pallas as pl
from jax.experimental.pallas import tpu as pltpu
from jax.sharding import PartitionSpec as P

HEAD = 128
SPAN = 128
TOK_DEV = 128
STAGES = 4
PIECES = 4
STEP = 512
TILE = 16

NORM_EPS = 1e-06
SWISH_ALPHA = 1.702
CLAMP_LIMIT = 7.0
MESH = pl.DeviceIdType.MESH
VMEM = pltpu.VMEM
DMA = pltpu.SemaphoreType.DMA
NT = (((1,), (1,)), ((), ()))
TN = (((0,), (0,)), ((), ()))


def remote(src, dst, send, recv, where):
    return pltpu.make_async_remote_copy(
        src_ref=src, dst_ref=dst, send_sem=send, recv_sem=recv, device_id=where, device_id_type=MESH
    )


def clamped_unit(gate, upward):
    glued = jnp.minimum(gate, CLAMP_LIMIT)
    linear = jnp.clip(upward, -CLAMP_LIMIT, CLAMP_LIMIT)
    return glued * jax.nn.sigmoid(SWISH_ALPHA * glued) * (linear + 1.0)


def rms_scale(values, gain):
    return values * lax.rsqrt(jnp.mean(values * values, axis=-1, keepdims=True) + NORM_EPS) * gain


def span_step(t, probe, ret, val, margin, extra, raw, qdec, state, running):
    rows = pl.ds(pl.multiple_of(t * SPAN, SPAN), SPAN)
    width = probe.shape[1]
    x = probe[rows, :].astype(jnp.float32)
    q = x * jax.nn.sigmoid(x) * HEAD ** (-0.5)
    k = margin[...] * jax.nn.sigmoid(-ret[rows, :].astype(jnp.float32))
    logs = jnp.log1p(-k)
    row = lax.broadcasted_iota(jnp.int32, (SPAN, SPAN), 0)
    col = lax.broadcasted_iota(jnp.int32, (SPAN, SPAN), 1)
    causal = row >= col
    tril = jnp.where(causal, 1.0, 0.0).astype(jnp.float32)
    for h in range(width // HEAD):
        cols = slice(h * HEAD, (h + 1) * HEAD)
        qh, kh = q[:, cols], k[:, cols]
        fade = jnp.transpose(jnp.broadcast_to(extra[h : h + 1, rows], (SPAN, SPAN)))
        ld = logs[:, cols] + fade
        cum = jnp.dot(
            tril, ld, precision=lax.Precision.HIGHEST, preferred_element_type=jnp.float32
        )
        middle = cum[SPAN // 2 - 1 : SPAN // 2, :]
        last = cum[SPAN - 1 :, :]
        a = (qh * jnp.exp(cum - middle)).astype(jnp.bfloat16)
        b = (kh * jnp.exp(middle - cum)).astype(jnp.bfloat16)
        qe = qh * jnp.exp(cum)
        kd = (kh * jnp.exp(last - cum)).astype(jnp.bfloat16)
        v = val[rows, cols]
        s = lax.dot_general(a, b, NT, preferred_element_type=jnp.float32)
        s = jnp.where(causal, s, 0.0).astype(jnp.bfloat16)
        st = state[h]
        out = jnp.dot(s, v, preferred_element_type=jnp.float32)
        out = out + lax.dot_general(
            qe.astype(jnp.bfloat16), st.astype(jnp.bfloat16), NT, preferred_element_type=jnp.float32
        )
        raw[rows, cols] = out
        before = running[0:1, cols]
        qdec[rows, cols] = (qe * jnp.exp(before)).astype(jnp.bfloat16)
        state[h] = jnp.exp(last) * st + lax.dot_general(
            v, kd, TN, preferred_element_type=jnp.float32
        )
        running[:, cols] = running[:, cols] + last


def kernel(
    n, planes, capacity, experts, named_by, shared_by, margin, extra, scale, lead, trail,
    tok_hbm, probe_hbm, ret_hbm, val_hbm, switch_hbm, mix_hbm, gate_hbm, up_hbm, down_hbm,
    mix_out, moe_out,
    nt, probe, ret, val, switch, mix_w, gate_w, up_w, down_w,
    rk, sh, meta, relay, meta2, relay2, rows, part, acc, sendb, recvb, fin, back, pk, pk2, pko, comb, spread,
    raw, qdec, state, state_bf, running, plst, pld, chain_in, chain_out, enter, carry, gath,
    load_sem,
    fsend, frecv, msend, mrecv, ysend, yrecv, zsend, zrecv, tsend, trecv, vsend, vrecv,
    xsend, xrecv, csend, crecv, dsend, drecv,
    esend0, erecv0, esend1, erecv1, bsend, brecv, rsend, rrecv,
    pssend, psrecv, pdsend, pdrecv, chsend, chrecv,
    gxsend, gxrecv, gcsend, gcrecv, gdsend, gdrecv,
):
    i, j = lax.axis_index("ep"), lax.axis_index("tp")
    mate = j + 1 - 2 * (j % 2)
    cross = (j + 2) % 4
    mate_cross = (mate + 2) % 4
    group = n // planes
    p, g = i // group, i % group
    features = nt.shape[2]
    heads = state.shape[0]
    width = probe.shape[1]
    length = probe.shape[0]
    f32, bf = jnp.float32, jnp.bfloat16

    pairs = (
        (tok_hbm, nt), (probe_hbm, probe), (ret_hbm, ret), (val_hbm, val),
        (gate_hbm, gate_w), (up_hbm, up_w), (down_hbm, down_w),
        (switch_hbm, switch), (mix_hbm, mix_w),
    )
    loads = [pltpu.make_async_copy(a, b, load_sem.at[w]) for w, (a, b) in enumerate(pairs)]
    for load in loads:
        load.start()

    barrier = pltpu.get_barrier_semaphore()

    def hello(s, c):
        pl.semaphore_signal(barrier, inc=1, device_id=((i + s) % n, j), device_id_type=MESH)
        return c

    lax.fori_loop(1, n, hello, 0)
    for t in (mate, cross):
        pl.semaphore_signal(barrier, inc=1, device_id=(i, t), device_id_type=MESH)

    def plane(s):
        left, right = p, planes - 1 - p
        big = (left - right + planes) // planes
        small = big * right + (1 - big) * left
        t = s - 1 + 2 * planes
        both = 1 - (t - 2 * small) // (2 * planes)
        t = t - 2 * planes
        far = both * ((t + 2) // 2) + (1 - both) * (s - small)
        sign = (2 * big - 1) * (2 * both * (s % 2) - 1)
        other = (s + planes - 1) // planes - s // planes
        return p + other * sign * far

    def place(c):
        t = (c + 1) // group
        last = (t + 1) // planes
        s = t + (t + planes - 1) // planes - last * (planes - 1)
        q = plane(s)
        return s, q, q * group + (g + (c + 1) % group) % group

    def ranks():
        ids = lax.broadcasted_iota(jnp.int32, (experts, TOK_DEV), 0)
        one = lax.broadcasted_iota(jnp.int32, (TOK_DEV, TOK_DEV), 0)
        two = lax.broadcasted_iota(jnp.int32, (TOK_DEV, TOK_DEV), 1)
        earlier = jnp.where(one < two, 1.0, 0.0).astype(bf)
        top = named_by.shape[0]
        for b in range(4):
            lanes = slice(b * TOK_DEV, (b + 1) * TOK_DEV)
            named = jnp.zeros((experts, TOK_DEV), f32)
            share = jnp.zeros((experts, TOK_DEV), f32)
            for w in range(top):
                hit = ids == named_by[w : w + 1, lanes]
                named = named + jnp.where(hit, 1.0, 0.0)
                share = share + jnp.where(hit, shared_by[w : w + 1, lanes], 0.0)
            ahead = jnp.dot(named.astype(bf), earlier, preferred_element_type=f32)
            rk[b] = jnp.where(named > 0.5, ahead, -1.0)
            sh[b] = share

    def norm(b):
        def tile(t, c):
            r = pl.ds(pl.multiple_of(t * TILE, TILE), TILE)
            nt[b, r, :] = rms_scale(nt[b, r, :].astype(f32), lead[...]).astype(bf)
            return c

        lax.fori_loop(0, TOK_DEV // TILE, tile, 0)

    slot = lax.broadcasted_iota(jnp.int32, (capacity, TOK_DEV), 0).astype(f32)

    def one_hot(ranked, e):
        return jnp.where(slot == ranked[pl.ds(e, 1), :], 1.0, 0.0)

    def pack(ranked, tokens, own, others):
        picks = [one_hot(ranked, i)]
        if others is not None:
            picks += [one_hot(ranked, p * group + (g + r) % group) for r in range(1, group)]
        pick = (picks[0] if len(picks) == 1 else jnp.concatenate(picks, axis=0)).astype(bf)
        for f in range(0, features, STEP):
            y = jnp.dot(pick, tokens[:, f : f + STEP], preferred_element_type=f32).astype(bf)
            own[:, f : f + STEP] = y[:capacity]
            for r in range(1, len(picks)):
                others[r - 1, :, f : f + STEP] = y[r * capacity : (r + 1) * capacity]

    def step_right(q, src, info):
        return (
            remote(src, relay.at[q], fsend.at[0, q], frecv.at[q], (i + group, j)),
            remote(info, meta.at[q], msend.at[0, q], mrecv.at[q], (i + group, j)),
        )

    def step_left(q, src, info):
        return (
            remote(src, relay.at[q], fsend.at[1, q], frecv.at[q], (i - group, j)),
            remote(info, meta.at[q], msend.at[1, q], mrecv.at[q], (i - group, j)),
        )

    def over_y(q, r):
        k = q * group + g
        d = p * group + (g + r) % group
        return remote(pk.at[q, r - 1], rows.at[k, j], ysend.at[q, r], yrecv.at[k], (d, j))

    def got_y(k):
        return remote(pk.at[0, 0], rows.at[k, j], ysend.at[0, 0], yrecv.at[k], (i, mate))

    def near(r, w):
        d = p * group + (g + r) % group
        b = (j, cross)[w]
        return remote(pko.at[w, r - 1], rows.at[i, b], zsend.at[w, r], zrecv.at[w, i], (d, j))

    def got_near(k, w):
        b = (j, cross)[w]
        return remote(pko.at[w, 0], rows.at[k, b], zsend.at[w, 0], zrecv.at[w, k], (i, mate))

    def over_x(k):
        return remote(rows.at[k, j], rows.at[k, j], xsend.at[k], xrecv.at[k], (i, cross))

    def over_c(k):
        return remote(rows.at[k, j], rows.at[k, j], csend.at[k], crecv.at[k], (i, mate))

    def over_d(k):
        return remote(rows.at[k, cross], rows.at[k, cross], dsend.at[k], drecv.at[k], (i, mate))

    def to_mate(k, close):
        if close:
            return remote(part.at[k, mate], acc.at[0, k], esend0.at[k], erecv0.at[k], (i, mate))
        return remote(
            part.at[k, mate_cross], acc.at[1, k], esend1.at[k], erecv1.at[k], (i, mate)
        )

    def to_cross(k):
        return remote(sendb.at[k], recvb.at[k], bsend.at[k], brecv.at[k], (i, cross))

    def home(k):
        return remote(fin.at[k], back.at[i], rsend.at[k], rrecv.at[i], (k, j))

    def home_in(k):
        return remote(fin.at[k], back.at[k], rsend.at[k], rrecv.at[k], (k, j))

    def twin():
        q = plane(1)
        return (
            remote(nt.at[cross], relay2, tsend.at[0], trecv.at[0], (q * group + g, j)),
            remote(rk.at[cross], meta2, tsend.at[1], trecv.at[1], (q * group + g, j)),
        )

    def twin_y(r):
        k = plane(1) * group + g
        d = p * group + (g + r) % group
        return remote(pk2.at[r - 1], rows.at[k, cross], vsend.at[r], vrecv.at[k], (d, j))

    def got_twin_y(k):
        return remote(pk2.at[0], rows.at[k, cross], vsend.at[0], vrecv.at[k], (i, mate))

    inner = (p >= 1) & (p + 1 < planes)

    def forward(s):
        q = plane(s)

        @pl.when(inner)
        def _():
            for copy in step_right(q, relay.at[q], meta.at[q]):
                copy.wait_recv()

        @pl.when(inner & (q < p))
        def _():
            for copy in step_right(q, relay.at[q], meta.at[q]):
                copy.start()

        @pl.when(inner & (q > p))
        def _():
            for copy in step_left(q, relay.at[q], meta.at[q]):
                copy.start()

    def arrive(s):
        q = plane(s)
        k = q * group + g

        @pl.when((p == 0) | (p + 1 == planes))
        def _():
            for copy in step_right(q, relay.at[q], meta.at[q]):
                copy.wait_recv()

        pack(meta.at[q], relay.at[q], rows.at[k, j], pk.at[q])

        @pl.when(s >= 2)
        def _():
            over_x(k).start()

        over_c(k).start()
        for r in range(1, group):
            over_y(q, r).start()

    def arrive_y(s):
        q = plane(s)
        for r in range(1, group):
            k = q * group + (g + r) % group
            got_y(k).wait_recv()

            @pl.when(s >= 2)
            def _():
                over_x(k).start()

            over_c(k).start()

    def arrive_twin():
        k = plane(1) * group + g
        for copy in twin():
            copy.wait_recv()
        pack(meta2, relay2, rows.at[k, cross], pk2)
        over_d(k).start()
        for r in range(1, group):
            twin_y(r).start()

    def arrive_twin_y():
        for r in range(1, group):
            k = plane(1) * group + (g + r) % group
            got_twin_y(k).wait_recv()
            over_d(k).start()

    def expert(k):
        x = rows[k].reshape(4 * capacity, features)
        gate = jnp.dot(x, gate_w[...], preferred_element_type=f32)
        upward = jnp.dot(x, up_w[...], preferred_element_type=f32)
        act = clamped_unit(gate, upward).astype(bf)
        for f in range(0, features, STEP):
            y = jnp.dot(act, down_w[:, f : f + STEP], preferred_element_type=f32)
            part[k, :, :, f : f + STEP] = y.astype(bf).reshape(4, capacity, STEP)
        to_mate(k, False).start()
        to_mate(k, True).start()

    def work(k, s):
        @pl.when(s >= 2)
        def _():
            over_x(k).wait_recv()
            over_d(k).start()

        over_c(k).wait_recv()
        over_d(k).wait_recv()
        expert(k)

    def first_sum(k):
        to_mate(k, False).wait()
        x = part[k, cross].astype(f32) + acc[1, k].astype(f32)
        sendb[k] = x.astype(bf)
        to_cross(k).start()

    def total(k):
        to_mate(k, True).wait()
        to_cross(k).wait()
        x = part[k, j].astype(f32) + acc[0, k].astype(f32)
        return (x + recvb[k].astype(f32)).astype(bf)

    def in_plane(r):
        d = p * group + (g + r) % group
        return (
            remote(state_bf, plst.at[g], pssend.at[r], psrecv.at[g], (d, j)),
            remote(running, pld.at[g], pdsend.at[r], pdrecv.at[g], (d, j)),
        )

    def in_plane_got(r):
        o = (g + r) % group
        return (
            remote(state_bf, plst.at[o], pssend.at[r], psrecv.at[o], (i, mate)),
            remote(running, pld.at[o], pdsend.at[r], pdrecv.at[o], (i, mate)),
        )

    def chain():
        return remote(chain_out, chain_in, chsend, chrecv, (i + group, j))

    def prefix():
        for r in range(1, group):
            for copy in in_plane_got(r):
                copy.wait_recv()

        @pl.when(p == 0)
        def _():
            carry[...] = jnp.zeros_like(carry)

        @pl.when(p >= 1)
        def _():
            chain().wait_recv()
            carry[...] = chain_in[...].astype(f32)

        for o in range(group):
            @pl.when(g == o)
            def _():
                enter[...] = carry[...]

            for h in range(heads):
                d = pld[o, 0:1, h * HEAD : (h + 1) * HEAD]
                carry[h] = jnp.exp(d) * carry[h] + plst[o, h].astype(f32)

        @pl.when(p + 1 < planes)
        def _():
            chain_out[...] = carry[...].astype(bf)
            chain().start()

    piece = length // PIECES

    def at(c):
        return pl.ds(pl.multiple_of(c * piece, piece), piece)

    def mix_x(c):
        here = gath.at[j, at(c)]
        return remote(here, here, gxsend.at[c], gxrecv.at[c], (i, cross))

    def mix_c(c):
        here = gath.at[j, at(c)]
        return remote(here, here, gcsend.at[c], gcrecv.at[c], (i, mate))

    def mix_d(c):
        here = gath.at[cross, at(c)]
        return remote(here, here, gdsend.at[c], gdrecv.at[c], (i, mate))

    def mix_final(c, z):
        r = at(c)
        for h in range(heads):
            cols = slice(h * HEAD, (h + 1) * HEAD)
            x = raw[r, cols] + lax.dot_general(
                qdec[r, cols], enter[h].astype(bf), NT, preferred_element_type=f32
            )
            x = x * lax.rsqrt(jnp.mean(x * x, axis=-1, keepdims=True) + NORM_EPS)
            v = switch[r, cols].astype(f32)
            gath[j, r, cols] = (x * scale[:, cols] * (v * jax.nn.sigmoid(v))).astype(bf)
        mix_x(c).start()
        mix_c(c).start()
        return z

    def mix_pass(c, z):
        mix_x(c).wait()
        mix_d(c).start()
        return z

    def mix_project(c, z):
        mix_c(c).wait()
        mix_d(c).wait()
        r = at(c)
        a = jnp.dot(gath[0, r, :], mix_w[0:width, :], preferred_element_type=f32)
        for w in range(1, 4):
            a = a + jnp.dot(
                gath[w, r, :], mix_w[w * width : (w + 1) * width, :], preferred_element_type=f32
            )
        mix_out[r, :] = a.astype(bf)
        return z

    ranks()
    loads[0].wait()
    norm(j)
    pl.semaphore_wait(barrier, n + 1)

    @pl.when(p + 1 < planes)
    def _():
        for copy in step_right(p, nt.at[j], rk.at[j]):
            copy.start()

    @pl.when(p >= 1)
    def _():
        for copy in step_left(p, nt.at[j], rk.at[j]):
            copy.start()

    norm(cross)
    for w, b in enumerate((j, cross)):
        pack(rk.at[b], nt.at[b], rows.at[i, b], pko.at[w])
        for r in range(1, group):
            near(r, w).start()
    norm(mate)
    norm(mate_cross)
    for b in (mate, mate_cross):
        pack(rk.at[b], nt.at[b], rows.at[i, b], None)

    for load in loads[1:4]:
        load.wait()
    state[...] = jnp.zeros_like(state)
    running[...] = jnp.zeros_like(running)

    def spans(t, c):
        span_step(t, probe, ret, val, margin, extra, raw, qdec, state, running)
        return c

    half = length // SPAN // 2
    for load in loads[4:]:
        load.wait()
    expert(i)
    first_sum(i)
    lax.fori_loop(0, half, spans, 0)
    if planes > 1:
        forward(1)
    lax.fori_loop(half, length // SPAN, spans, 0)
    for h in range(heads):
        state_bf[h] = state[h].astype(bf)
    plst[g] = state_bf[...]
    pld[g] = running[...]
    for r in range(1, group):
        for copy in in_plane(r):
            copy.start()
    for r in range(1, group):
        k = p * group + (g + r) % group
        got_near(k, 0).wait_recv()
        over_c(k).start()
        got_near(k, 1).wait_recv()
        over_d(k).start()

    def turn(u):
        return u - (u + n - group) // n

    def pump(u, z):
        @pl.when(u < planes - 2)
        def _():
            forward(u + 2)

        @pl.when(u == 1)
        def _():
            for copy in twin():
                copy.start()

        @pl.when((u < n) & (u != group - 1))
        def _():
            s, q, k = place(turn(u))
            work(k, s)
            first_sum(k)

        @pl.when(u < planes - 1)
        def _():
            arrive(u + 1)

        @pl.when((u >= 1) & (u < n + 1) & (u != group))
        def _():
            s, q, k = place(turn(u - 1))
            fin[k] = total(k)
            home(k).start()

        @pl.when(u == 0)
        def _():
            back[i] = total(i)
            prefix()

        @pl.when(u < planes - 1)
        def _():
            arrive_y(u + 1)

        @pl.when(u == planes)
        def _():
            arrive_twin()

        @pl.when(u == planes + 1)
        def _():
            arrive_twin_y()

        @pl.when(u == n - 1)
        def _():
            lax.fori_loop(0, PIECES, mix_final, 0)

        return z

    lax.fori_loop(0, n + 1, pump, 0)
    lax.fori_loop(0, PIECES, mix_pass, 0)
    lax.fori_loop(0, PIECES, mix_project, 0)

    def weigh(e, z):
        r = pl.ds(pl.multiple_of(e * capacity, capacity), capacity)
        spread[r, :] = jnp.where(
            slot == rk[j, pl.ds(e, 1), :], jnp.broadcast_to(sh[j, pl.ds(e, 1), :], slot.shape), 0.0
        )
        return z

    lax.fori_loop(0, experts, weigh, 0)
    wide = spread[...]
    high = wide.astype(bf)
    low = (wide - high.astype(f32)).astype(bf)

    def collect(s, z):
        k = (i + s) % n
        home_in(k).wait_recv()
        return z

    lax.fori_loop(1, n, collect, 0)
    for f in range(0, features, STEP):
        flat = back[:, :, f : f + STEP].reshape(n * capacity, STEP)
        comb[:, f : f + STEP] = lax.dot_general(
            high, flat, TN, preferred_element_type=f32
        ) + lax.dot_general(low, flat, TN, preferred_element_type=f32)

    def closing(t, z):
        r = pl.ds(pl.multiple_of(t * TILE, TILE), TILE)
        moe_out[r, :] = rms_scale(comb[r, :], trail[...]).astype(bf)
        return z

    lax.fori_loop(0, TOK_DEV // TILE, closing, 0)

    def finish(s, z):
        k = (i + s) % n
        over_c(k).wait_send()
        over_d(k).wait_send()
        home(k).wait_send()
        return z

    lax.fori_loop(1, n, finish, 0)

    def finish_far(s, z):
        q = plane(s)

        @pl.when(s >= 2)
        def _():
            for r in range(group):
                over_x(q * group + r).wait_send()

        for r in range(1, group):
            over_y(q, r).wait_send()

        @pl.when((q < p) & (p + 1 < planes))
        def _():
            for copy in step_right(q, relay.at[q], meta.at[q]):
                copy.wait_send()

        @pl.when((q > p) & (p >= 1))
        def _():
            for copy in step_left(q, relay.at[q], meta.at[q]):
                copy.wait_send()

        return z

    lax.fori_loop(1, planes, finish_far, 0)

    @pl.when(p + 1 < planes)
    def _():
        for copy in step_right(p, nt.at[j], rk.at[j]):
            copy.wait_send()
        chain().wait_send()

    @pl.when(p >= 1)
    def _():
        for copy in step_left(p, nt.at[j], rk.at[j]):
            copy.wait_send()

    if planes > 1:
        for copy in twin():
            copy.wait_send()
        for r in range(1, group):
            twin_y(r).wait_send()
    for r in range(1, group):
        for w in range(2):
            near(r, w).wait_send()
        for copy in in_plane(r):
            copy.wait_send()


def shards(
    state_probe_logits,
    retention_logits,
    state_source_entries,
    state_result_switch_logits,
    retention_bound_margin,
    extra_fading_amount,
    state_result_scale,
    state_result_matrix,
    second_slice_tokens,
    specialist_assignment,
    selected_specialist_share,
    leading_scale_vector,
    trailing_scale_vector,
    specialist_switch_matrix,
    specialist_widen_matrix,
    specialist_contract_matrix,
):
    n = lax.axis_size("ep")
    experts = specialist_switch_matrix.shape[0] * n
    top_count = specialist_assignment.shape[1]
    capacity = 2 * TOK_DEV * top_count // experts
    planes = max(d for d in (1, 2, STAGES) if n % (2 * d) == 0)
    group = n // planes
    length, width = state_probe_logits.shape
    heads = width // HEAD
    features = second_slice_tokens.shape[1]
    hidden = specialist_switch_matrix.shape[2]
    columns = state_result_matrix.shape[1]
    bf, f32 = jnp.bfloat16, jnp.float32
    vm = pl.BlockSpec(memory_space=VMEM)
    hbm = pl.BlockSpec(memory_space=pl.ANY)
    chunk = (capacity, features)
    block = (TOK_DEV, features)
    return tuple(
        pl.pallas_call(
            functools.partial(kernel, n, planes, capacity, experts),
            name="fused",
            out_shape=(
                jax.ShapeDtypeStruct((length, columns), bf),
                jax.ShapeDtypeStruct(block, bf),
            ),
            in_specs=[vm] * 7 + [hbm] * 9,
            out_specs=(vm, vm),
            scratch_shapes=[
                VMEM((4,) + block, bf),
                VMEM((length, width), bf),
                VMEM((length, width), bf),
                VMEM((length, width), bf),
                VMEM((length, width), bf),
                VMEM(state_result_matrix.shape, bf),
                VMEM((features, hidden), bf),
                VMEM((features, hidden), bf),
                VMEM((hidden, features), bf),
                VMEM((4, experts, TOK_DEV), f32),
                VMEM((4, experts, TOK_DEV), f32),
                VMEM((planes, experts, TOK_DEV), f32),
                VMEM((planes,) + block, bf),
                VMEM((experts, TOK_DEV), f32),
                VMEM(block, bf),
                VMEM((n, 4) + chunk, bf),
                VMEM((n, 4) + chunk, bf),
                VMEM((2, n) + chunk, bf),
                VMEM((n,) + chunk, bf),
                VMEM((n,) + chunk, bf),
                VMEM((n,) + chunk, bf),
                VMEM((n,) + chunk, bf),
                VMEM((planes, group - 1) + chunk, bf),
                VMEM((group - 1,) + chunk, bf),
                VMEM((2, group - 1) + chunk, bf),
                VMEM(block, f32),
                VMEM((n * capacity, TOK_DEV), f32),
                VMEM((length, width), f32),
                VMEM((length, width), bf),
                VMEM((heads, HEAD, HEAD), f32),
                VMEM((heads, HEAD, HEAD), bf),
                VMEM((8, width), f32),
                VMEM((group, heads, HEAD, HEAD), bf),
                VMEM((group, 8, width), f32),
                VMEM((heads, HEAD, HEAD), bf),
                VMEM((heads, HEAD, HEAD), bf),
                VMEM((heads, HEAD, HEAD), f32),
                VMEM((heads, HEAD, HEAD), f32),
                VMEM((4, length, width), bf),
                DMA((9,)),
                DMA((2, planes)), DMA((planes,)), DMA((2, planes)), DMA((planes,)),
                DMA((planes, group)), DMA((n,)), DMA((2, group)), DMA((2, n)),
                DMA((2,)), DMA((2,)), DMA((group,)), DMA((n,)),
            ]
            + [DMA((n,))] * 14
            + [DMA((group,))] * 4
            + [DMA, DMA]
            + [DMA((PIECES,))] * 6,
            compiler_params=pltpu.CompilerParams(
                collective_id=0, has_side_effects=True, vmem_limit_bytes=62 * 2**20
            ),
        )(
            specialist_assignment.T,
            selected_specialist_share.T,
            retention_bound_margin[None, :],
            extra_fading_amount.T,
            state_result_scale[None, :],
            leading_scale_vector[None, :],
            trailing_scale_vector[None, :],
            second_slice_tokens.reshape((4,) + block),
            state_probe_logits,
            retention_logits,
            state_source_entries,
            state_result_switch_logits,
            state_result_matrix,
            specialist_switch_matrix[0],
            specialist_widen_matrix[0],
            specialist_contract_matrix[0],
        )
    )


def solution(mesh):
    return jax.shard_map(
        shards,
        mesh=mesh,
        in_specs=(
            P("ep", "tp"),
            P("ep", "tp"),
            P("ep", "tp"),
            P("ep", "tp"),
            P("tp"),
            P("ep", "tp"),
            P("tp"),
            P(None, "tp"),
            P("ep", None),
            P("ep", None),
            P("ep", None),
            P(),
            P(),
            P("ep", None, "tp"),
            P("ep", None, "tp"),
            P("ep", "tp", None),
        ),
        out_specs=(P("ep", "tp"), P(("ep", "tp"), None)),
        check_vma=False,
    )
```

```python
import functools

import jax
import jax.numpy as jnp
from jax import lax
from jax.experimental import pallas as pl
from jax.experimental.pallas import tpu as pltpu
from jax.sharding import PartitionSpec as P

HEAD = 128
SPAN = 128
TOK_DEV = 128
STAGES = 4
PIECES = 4
STEP = 512
TILE = 16
LIMIT = 62

NORM_EPS = 1e-06
SWISH_ALPHA = 1.702
CLAMP_LIMIT = 7.0
MESH = pl.DeviceIdType.MESH
VMEM = pltpu.VMEM
DMA = pltpu.SemaphoreType.DMA
NT = (((1,), (1,)), ((), ()))
TN = (((0,), (0,)), ((), ()))


def remote(src, dst, send, recv, where):
    return pltpu.make_async_remote_copy(
        src_ref=src, dst_ref=dst, send_sem=send, recv_sem=recv, device_id=where, device_id_type=MESH
    )


def clamped_unit(gate, upward):
    glued = jnp.minimum(gate, CLAMP_LIMIT)
    linear = jnp.clip(upward, -CLAMP_LIMIT, CLAMP_LIMIT)
    return glued * jax.nn.sigmoid(SWISH_ALPHA * glued) * (linear + 1.0)


def rms_scale(values, gain):
    return values * lax.rsqrt(jnp.mean(values * values, axis=-1, keepdims=True) + NORM_EPS) * gain


def span_step(t, probe, ret, val, margin, extra, raw, qdec, state, running):
    rows = pl.ds(pl.multiple_of(t * SPAN, SPAN), SPAN)
    width = probe.shape[1]
    x = probe[rows, :].astype(jnp.float32)
    q = x * jax.nn.sigmoid(x) * HEAD ** (-0.5)
    k = margin[...] * jax.nn.sigmoid(-ret[rows, :].astype(jnp.float32))
    logs = jnp.log1p(-k)
    row = lax.broadcasted_iota(jnp.int32, (SPAN, SPAN), 0)
    col = lax.broadcasted_iota(jnp.int32, (SPAN, SPAN), 1)
    causal = row >= col
    tril = jnp.where(causal, 1.0, 0.0).astype(jnp.float32)
    for h in range(width // HEAD):
        cols = slice(h * HEAD, (h + 1) * HEAD)
        qh, kh = q[:, cols], k[:, cols]
        fade = jnp.transpose(jnp.broadcast_to(extra[h : h + 1, rows], (SPAN, SPAN)))
        ld = logs[:, cols] + fade
        cum = jnp.dot(
            tril, ld, precision=lax.Precision.HIGHEST, preferred_element_type=jnp.float32
        )
        middle = cum[SPAN // 2 - 1 : SPAN // 2, :]
        last = cum[SPAN - 1 :, :]
        a = (qh * jnp.exp(cum - middle)).astype(jnp.bfloat16)
        b = (kh * jnp.exp(middle - cum)).astype(jnp.bfloat16)
        qe = qh * jnp.exp(cum)
        kd = (kh * jnp.exp(last - cum)).astype(jnp.bfloat16)
        v = val[rows, cols]
        s = lax.dot_general(a, b, NT, preferred_element_type=jnp.float32)
        s = jnp.where(causal, s, 0.0).astype(jnp.bfloat16)
        st = state[h]
        out = jnp.dot(s, v, preferred_element_type=jnp.float32)
        out = out + lax.dot_general(
            qe.astype(jnp.bfloat16), st.astype(jnp.bfloat16), NT, preferred_element_type=jnp.float32
        )
        raw[rows, cols] = out
        before = running[0:1, cols]
        qdec[rows, cols] = (qe * jnp.exp(before)).astype(jnp.bfloat16)
        state[h] = jnp.exp(last) * st + lax.dot_general(
            v, kd, TN, preferred_element_type=jnp.float32
        )
        running[:, cols] = running[:, cols] + last


def kernel(
    n, planes, capacity, experts,
    named_hbm, shared_hbm, margin_hbm, extra_hbm, scale_hbm, lead_hbm, trail_hbm, tok_hbm, probe_hbm, ret_hbm, val_hbm, switch_hbm, mix_hbm, gate_hbm, up_hbm, down_hbm,
    mix_hbm_out, moe_hbm_out,
    mix_out, moe_out,
    named_by, shared_by, margin, extra, scale, lead, trail, nt, probe, ret, val, switch, mix_w, gate_w, up_w, down_w,
    rk, sh, meta, relay, meta2, relay2, rows, part, acc, sendb, recvb, back, pk, pk2, pko, comb, spread, share_hi, share_lo,
    raw, qdec, state, state_bf, running, plst, pld, chain_in, chain_out, enter, carry, gath,
    load_sem, store_sem, moe_sem,
    fsend, frecv, msend, mrecv, ysend, yrecv, zsend, zrecv, tsend, trecv, vsend, vrecv, qsend, qrecv,
    xsend, xrecv, csend, crecv, dsend, drecv,
    esend0, erecv0, esend1, erecv1, bsend, brecv, rsend, rrecv,
    pssend, psrecv, pdsend, pdrecv, chsend, chrecv,
    gxsend, gxrecv, gcsend, gcrecv, gdsend, gdrecv,
):
    i, j = lax.axis_index("ep"), lax.axis_index("tp")
    mate = j + 1 - 2 * (j % 2)
    cross = (j + 2) % 4
    mate_cross = (mate + 2) % 4
    group = n // planes
    p, g = i // group, i % group
    features = nt.shape[2]
    heads = state.shape[0]
    width = probe.shape[1]
    length = probe.shape[0]
    f32, bf = jnp.float32, jnp.bfloat16

    pairs = (
        (tok_hbm, nt), (lead_hbm, lead), (named_hbm, named_by), (shared_hbm, shared_by),
        (margin_hbm, margin), (extra_hbm, extra),
        (probe_hbm, probe), (ret_hbm, ret), (val_hbm, val),
        (gate_hbm, gate_w), (up_hbm, up_w), (down_hbm, down_w),
        (switch_hbm, switch), (mix_hbm, mix_w), (scale_hbm, scale), (trail_hbm, trail),
    )
    loads = [pltpu.make_async_copy(a, b, load_sem.at[w]) for w, (a, b) in enumerate(pairs)]
    for load in loads:
        load.start()

    barrier = pltpu.get_barrier_semaphore()

    def hello(s, c):
        pl.semaphore_signal(barrier, inc=1, device_id=((i + s) % n, j), device_id_type=MESH)
        return c

    lax.fori_loop(1, n, hello, 0)
    for t in (mate, cross):
        pl.semaphore_signal(barrier, inc=1, device_id=(i, t), device_id_type=MESH)
    for r in range(1, group):
        d = p * group + (g + r) % group
        pl.semaphore_signal(barrier, inc=1, device_id=(d, cross), device_id_type=MESH)

    more = (p + planes - 1) // planes
    less = (2 * planes - 2 - p) // planes
    early = more * less

    def plane(s):
        left, right = p, planes - 1 - p
        big = (left - right + planes) // planes
        small = big * right + (1 - big) * left
        t = s - 1 + 2 * planes
        both = 1 - (t - 2 * small) // (2 * planes)
        t = t - 2 * planes
        far = both * ((t + 2) // 2) + (1 - both) * (s - small)
        sign = (2 * big - 1) * (2 * both * (s % 2) - 1)
        other = (s + planes - 1) // planes - s // planes
        return p + other * sign * far

    half = max(group // 2, 1)

    def table(h, values):
        total = values[0]
        for v in range(1, len(values)):
            total = total + (values[v] - values[v - 1]) * ((h + len(values) - v) // len(values))
        return total

    def place(c):
        away = (c + 1 - group + n) // n
        rest = away * (c + 1 - group)
        h = rest // half
        inside = (table(h, (2, 2, 3, 3, 1, 1)), table(h, (0, 0, 2, 2, 4, 4)))
        outside = (table(h, (2, 2, 1, 3, 3, 1)), table(h, (0, 0, 2, 3, 3, 4)))
        s, base = (early * a + (1 - early) * b for a, b in zip(inside, outside))
        s = away * s
        r = away * (rest - half * base) + (1 - away) * (c + 1)
        q = plane(s)
        return s, r, q * group + (g + r) % group

    def ranks():
        ids = lax.broadcasted_iota(jnp.int32, (experts, TOK_DEV), 0)
        one = lax.broadcasted_iota(jnp.int32, (TOK_DEV, TOK_DEV), 0)
        two = lax.broadcasted_iota(jnp.int32, (TOK_DEV, TOK_DEV), 1)
        earlier = jnp.where(one < two, 1.0, 0.0).astype(bf)
        top = named_by.shape[0]
        for b in range(4):
            lanes = slice(b * TOK_DEV, (b + 1) * TOK_DEV)
            named = jnp.zeros((experts, TOK_DEV), f32)
            share = jnp.zeros((experts, TOK_DEV), f32)
            for w in range(top):
                hit = ids == named_by[w : w + 1, lanes]
                named = named + jnp.where(hit, 1.0, 0.0)
                share = share + jnp.where(hit, shared_by[w : w + 1, lanes], 0.0)
            ahead = jnp.dot(named.astype(bf), earlier, preferred_element_type=f32)
            rk[b] = jnp.where(named > 0.5, ahead, -1.0)
            sh[b] = share

    def norm(b):
        def tile(t, c):
            r = pl.ds(pl.multiple_of(t * TILE, TILE), TILE)
            nt[b, r, :] = rms_scale(nt[b, r, :].astype(f32), lead[...]).astype(bf)
            return c

        lax.fori_loop(0, TOK_DEV // TILE, tile, 0)

    slot = lax.broadcasted_iota(jnp.int32, (capacity, TOK_DEV), 0).astype(f32)

    def one_hot(ranked, e):
        return jnp.where(slot == ranked[pl.ds(e, 1), :], 1.0, 0.0)

    def pack(ranked, tokens, own, others):
        picks = [one_hot(ranked, i)]
        if others is not None:
            picks += [one_hot(ranked, p * group + (g + r) % group) for r in range(1, group)]
        pick = (picks[0] if len(picks) == 1 else jnp.concatenate(picks, axis=0)).astype(bf)
        for f in range(0, features, STEP):
            y = jnp.dot(pick, tokens[:, f : f + STEP], preferred_element_type=f32).astype(bf)
            own[:, f : f + STEP] = y[:capacity]
            for r in range(1, len(picks)):
                others[r - 1, :, f : f + STEP] = y[r * capacity : (r + 1) * capacity]

    def step_right(q, src, info):
        return (
            remote(src, relay.at[q], fsend.at[0, q], frecv.at[q], (i + group, j)),
            remote(info, meta.at[q], msend.at[0, q], mrecv.at[q], (i + group, j)),
        )

    def step_left(q, src, info):
        return (
            remote(src, relay.at[q], fsend.at[1, q], frecv.at[q], (i - group, j)),
            remote(info, meta.at[q], msend.at[1, q], mrecv.at[q], (i - group, j)),
        )

    def over_y(q, r):
        k = q * group + g
        d = p * group + (g + r) % group
        return remote(pk.at[q, r - 1], rows.at[k, j], ysend.at[q, r], yrecv.at[k], (d, j))

    def got_y(k):
        return remote(pk.at[0, 0], rows.at[k, j], ysend.at[0, 0], yrecv.at[k], (i, mate))

    def over_xy(q, r):
        k = q * group + g
        d = p * group + (g + r) % group
        return remote(pk.at[q, r - 1], rows.at[k, j], qsend.at[q, r], qrecv.at[k], (d, cross))

    def got_xy(k):
        return remote(pk.at[0, 0], rows.at[k, cross], qsend.at[0, 0], qrecv.at[k], (i, mate))

    def near(r, w):
        d = p * group + (g + r) % group
        b = (j, cross)[w]
        return remote(pko.at[w, r - 1], rows.at[i, b], zsend.at[w, r], zrecv.at[w, i], (d, j))

    def got_near(k, w):
        b = (j, cross)[w]
        return remote(pko.at[w, 0], rows.at[k, b], zsend.at[w, 0], zrecv.at[w, k], (i, mate))

    def over_x(k):
        return remote(rows.at[k, j], rows.at[k, j], xsend.at[k], xrecv.at[k], (i, cross))

    def over_c(k):
        return remote(rows.at[k, j], rows.at[k, j], csend.at[k], crecv.at[k], (i, mate))

    def over_d(k):
        return remote(rows.at[k, cross], rows.at[k, cross], dsend.at[k], drecv.at[k], (i, mate))

    def to_mate(k, close):
        if close:
            return remote(part.at[k, mate], acc.at[0, k], esend0.at[k], erecv0.at[k], (i, mate))
        return remote(
            part.at[k, mate_cross], acc.at[1, k], esend1.at[k], erecv1.at[k], (i, mate)
        )

    def to_cross(k):
        return remote(sendb.at[k], recvb.at[k], bsend.at[k], brecv.at[k], (i, cross))

    def home(k):
        return remote(sendb.at[k], back.at[i], rsend.at[k], rrecv.at[i], (k, j))

    def home_in(k):
        return remote(sendb.at[k], back.at[k], rsend.at[k], rrecv.at[k], (k, j))

    upper = 2 * p // planes
    source = (planes - 1) * (1 - upper)

    def twin(side, first):
        src = (nt.at[cross], rk.at[cross]) if first else (relay2.at[side], meta2.at[side])
        dst = (relay2.at[side], meta2.at[side])
        d = i + group - 2 * group * side
        return [
            remote(src[w], dst[w], tsend.at[side, w], trecv.at[side, w], (d, j)) for w in range(2)
        ]

    def twin_start():
        @pl.when(p == 0)
        def _():
            for copy in twin(0, True):
                copy.start()

        @pl.when(p == planes - 1)
        def _():
            for copy in twin(1, True):
                copy.start()

    def twin_pass(side, used):
        mine = (upper == 1) if side == 0 else (upper == 0)
        take = mine if used else jnp.logical_not(mine)
        reach = (p > 0) if side == 0 else (p < planes - 1)
        on = (p < planes - 1) if side == 0 else (p > 0)

        @pl.when(take & reach)
        def _():
            for copy in twin(side, False):
                copy.wait_recv()

        @pl.when(take & reach & on)
        def _():
            for copy in twin(side, False):
                copy.start()

    def twin_y(r):
        k = source * group + g
        d = p * group + (g + r) % group
        return remote(pk2.at[r - 1], rows.at[k, cross], vsend.at[r], vrecv.at[k], (d, j))

    def got_twin_y(k):
        return remote(pk2.at[0], rows.at[k, cross], vsend.at[0], vrecv.at[k], (i, mate))

    inner = (p >= 1) & (p + 1 < planes)

    def forward(s):
        q = plane(s)

        @pl.when(inner)
        def _():
            for copy in step_right(q, relay.at[q], meta.at[q]):
                copy.wait_recv()

        @pl.when(inner & (q < p))
        def _():
            for copy in step_right(q, relay.at[q], meta.at[q]):
                copy.start()

        @pl.when(inner & (q > p))
        def _():
            for copy in step_left(q, relay.at[q], meta.at[q]):
                copy.start()

    def direct(s):
        return (s >= 1) & (s < planes - 1) & (s > early)

    def late():
        q = plane(1)
        over_x(q * group + g).start()
        for r in range(1, group):
            k = q * group + (g + r) % group
            got_y(k).wait_recv()
            over_x(k).start()

    def arrive(s):
        q = plane(s)
        k = q * group + g

        @pl.when((p == 0) | (p + 1 == planes))
        def _():
            for copy in step_right(q, relay.at[q], meta.at[q]):
                copy.wait_recv()

        pack(meta.at[q], relay.at[q], rows.at[k, j], pk.at[q])

        @pl.when(direct(s))
        def _():
            over_x(k).start()
            for r in range(1, group):
                over_xy(q, r).start()

        for r in range(1, group):
            over_y(q, r).start()

    def arrive_twin():
        k = source * group + g
        for side in range(2):
            twin_pass(side, True)
        for side in range(2):

            @pl.when(upper == 1 - side)
            def _():
                pack(meta2.at[side], relay2.at[side], rows.at[k, cross], pk2)

        for r in range(1, group):
            twin_y(r).start()

    def expert(k):
        x = rows[k].reshape(4 * capacity, features)
        gate = jnp.dot(x, gate_w[...], preferred_element_type=f32)
        upward = jnp.dot(x, up_w[...], preferred_element_type=f32)
        act = clamped_unit(gate, upward).astype(bf)
        for f in range(0, features, STEP):
            y = jnp.dot(act, down_w[:, f : f + STEP], preferred_element_type=f32)
            part[k, :, :, f : f + STEP] = y.astype(bf).reshape(4, capacity, STEP)
        to_mate(k, False).start()
        to_mate(k, True).start()

    def prepare(c):
        s, r, k = place(c)

        @pl.when(s == 0)
        def _():
            got_near(k, 0).wait_recv()
            got_near(k, 1).wait_recv()

        @pl.when((r >= 1) & (direct(s) | ((s >= 1) & (s == planes - 1))))
        def _():
            got_y(k).wait_recv()

        @pl.when((s >= 1) & (s == planes - 1) & (r >= 1))
        def _():
            got_twin_y(k).wait_recv()

        @pl.when(direct(s) & (r >= 1))
        def _():
            got_xy(k).wait_recv()

        @pl.when((s >= 1) & (s < planes - 1) & ((r == 0) | (s <= early)))
        def _():
            over_x(k).wait_recv()

        over_c(k).start()
        over_d(k).start()

    def work(k):
        over_c(k).wait_recv()
        over_d(k).wait_recv()
        expert(k)

    def first_sum(k):
        to_mate(k, False).wait()
        x = part[k, cross].astype(f32) + acc[1, k].astype(f32)
        sendb[k] = x.astype(bf)
        to_cross(k).start()

    def total(k):
        to_mate(k, True).wait()
        to_cross(k).wait()
        x = part[k, j].astype(f32) + acc[0, k].astype(f32)
        return (x + recvb[k].astype(f32)).astype(bf)

    def in_plane(r):
        d = p * group + (g + r) % group
        return (
            remote(state_bf, plst.at[g], pssend.at[r], psrecv.at[g], (d, j)),
            remote(running, pld.at[g], pdsend.at[r], pdrecv.at[g], (d, j)),
        )

    def in_plane_got(r):
        o = (g + r) % group
        return (
            remote(state_bf, plst.at[o], pssend.at[r], psrecv.at[o], (i, mate)),
            remote(running, pld.at[o], pdsend.at[r], pdrecv.at[o], (i, mate)),
        )

    def chain():
        return remote(chain_out, chain_in, chsend, chrecv, (i + group, j))

    def prefix():
        for r in range(1, group):
            for copy in in_plane_got(r):
                copy.wait_recv()

        @pl.when(p == 0)
        def _():
            carry[...] = jnp.zeros_like(carry)

        @pl.when(p >= 1)
        def _():
            chain().wait_recv()
            carry[...] = chain_in[...].astype(f32)

        for o in range(group):
            @pl.when(g == o)
            def _():
                enter[...] = carry[...]

            for h in range(heads):
                d = pld[o, 0:1, h * HEAD : (h + 1) * HEAD]
                carry[h] = jnp.exp(d) * carry[h] + plst[o, h].astype(f32)

        @pl.when(p + 1 < planes)
        def _():
            chain_out[...] = carry[...].astype(bf)
            chain().start()

    piece = length // PIECES

    def at(c):
        return pl.ds(pl.multiple_of(c * piece, piece), piece)

    def mix_x(c):
        here = gath.at[j, at(c)]
        return remote(here, here, gxsend.at[c], gxrecv.at[c], (i, cross))

    def mix_c(c):
        here = gath.at[j, at(c)]
        return remote(here, here, gcsend.at[c], gcrecv.at[c], (i, mate))

    def mix_d(c):
        here = gath.at[cross, at(c)]
        return remote(here, here, gdsend.at[c], gdrecv.at[c], (i, mate))

    def store(c):
        return pltpu.make_async_copy(mix_out.at[at(c)], mix_hbm_out.at[at(c)], store_sem.at[c])

    def mix_final(c, z):
        r = at(c)
        for h in range(heads):
            cols = slice(h * HEAD, (h + 1) * HEAD)
            x = raw[r, cols] + lax.dot_general(
                qdec[r, cols], enter[h].astype(bf), NT, preferred_element_type=f32
            )
            x = x * lax.rsqrt(jnp.mean(x * x, axis=-1, keepdims=True) + NORM_EPS)
            v = switch[r, cols].astype(f32)
            gath[j, r, cols] = (x * scale[:, cols] * (v * jax.nn.sigmoid(v))).astype(bf)
        mix_x(c).start()
        mix_c(c).start()
        return z

    def mix_pass(c, z):
        mix_x(c).wait()
        mix_d(c).start()
        return z

    def mix_project(c, z):
        mix_c(c).wait()
        mix_d(c).wait()
        r = at(c)
        a = jnp.dot(gath[0, r, :], mix_w[0:width, :], preferred_element_type=f32)
        for w in range(1, 4):
            a = a + jnp.dot(
                gath[w, r, :], mix_w[w * width : (w + 1) * width, :], preferred_element_type=f32
            )
        mix_out[r, :] = a.astype(bf)
        store(c).start()
        return z

    for load in loads[2:4]:
        load.wait()
    ranks()
    for load in loads[:2]:
        load.wait()
    norm(j)
    pl.semaphore_wait(barrier, n + group)

    @pl.when(p + 1 < planes)
    def _():
        for copy in step_right(p, nt.at[j], rk.at[j]):
            copy.start()

    @pl.when(p >= 1)
    def _():
        for copy in step_left(p, nt.at[j], rk.at[j]):
            copy.start()

    norm(cross)
    if planes > 1:
        twin_start()
    for w, b in enumerate((j, cross)):
        pack(rk.at[b], nt.at[b], rows.at[i, b], pko.at[w])
        for r in range(1, group):
            near(r, w).start()
    norm(mate)
    norm(mate_cross)
    for b in (mate, mate_cross):
        pack(rk.at[b], nt.at[b], rows.at[i, b], None)

    for load in loads[4:9]:
        load.wait()
    state[...] = jnp.zeros_like(state)
    running[...] = jnp.zeros_like(running)

    def spans(t, c):
        span_step(t, probe, ret, val, margin, extra, raw, qdec, state, running)
        return c

    for load in loads[9:]:
        load.wait()
    expert(i)
    first_sum(i)
    lax.fori_loop(0, length // SPAN, spans, 0)
    for h in range(heads):
        state_bf[h] = state[h].astype(bf)
    plst[g] = state_bf[...]
    pld[g] = running[...]
    for r in range(1, group):
        for copy in in_plane(r):
            copy.start()
    for t in range(1, min(planes, 3)):
        forward(t)

    if planes > 1:
        @pl.when(early > 0)
        def _():
            arrive(2)

        arrive(1)
    prepare(0)

    def turn(u):
        return u - (1 - early) * ((u + n - group) // n)

    def busy(u):
        return (u >= 0) & (u < n - early) & ((early > 0) | (u != group - 1))

    def ready(u):
        @pl.when(busy(u))
        def _():
            prepare(turn(u))

    def pump(u, z):
        @pl.when((u >= 1) & (u < planes - 2))
        def _():
            forward(u + 2)

        @pl.when(u == 1)
        def _():
            for side in range(2):
                twin_pass(side, False)

        @pl.when(busy(u))
        def _():
            s, r, k = place(turn(u))
            work(k)
            first_sum(k)

        @pl.when(u == n - 1 - early)
        def _():
            lax.fori_loop(0, PIECES, mix_final, 0)

        if planes > 1:

            @pl.when((u == 1) | (u == 2 - early))
            def _():
                arrive(u + 1 + early)

            @pl.when(u == 12 * early - 9)
            def _():
                late()

        if planes > 1:

            @pl.when(u == 3 - early)
            def _():
                arrive_twin()

        @pl.when(u >= planes)
        def _():
            ready(u + 1)

        @pl.when(busy(u - 1))
        def _():
            s, r, k = place(turn(u - 1))
            sendb[k] = total(k)
            home(k).start()

        @pl.when(u == 0)
        def _():
            back[i] = total(i)
            weights()

        @pl.when(u == p)
        def _():
            prefix()

        @pl.when(u < planes)
        def _():
            ready(u + 1)

        return z

    def weights():
        lax.fori_loop(0, experts, weigh, 0)
        for b in range(n * capacity // TOK_DEV):
            wide = jnp.transpose(spread[b * TOK_DEV : (b + 1) * TOK_DEV, :])
            high = wide.astype(bf)
            share_hi[b] = high
            share_lo[b] = (wide - high.astype(f32)).astype(bf)

    def weigh(e, z):
        r = pl.ds(pl.multiple_of(e * capacity, capacity), capacity)
        spread[r, :] = jnp.where(
            slot == rk[j, pl.ds(e, 1), :], jnp.broadcast_to(sh[j, pl.ds(e, 1), :], slot.shape), 0.0
        )
        return z

    lax.fori_loop(0, n + 1, pump, 0)
    lax.fori_loop(0, PIECES, mix_pass, 0)
    lax.fori_loop(0, PIECES, mix_project, 0)

    def collect(s, first):
        q = plane(s)
        for r in range(group):
            k = q * group + (g + r) % group
            if not (first and r == 0):
                home_in(k).wait_recv()
        for f in range(0, features, STEP):
            flat = back[pl.ds(q * group, group), :, f : f + STEP].reshape(group * capacity, STEP)
            y = jnp.dot(share_hi[q], flat, preferred_element_type=f32) + jnp.dot(
                share_lo[q], flat, preferred_element_type=f32
            )
            comb[:, f : f + STEP] = y if first else comb[:, f : f + STEP] + y

    collect(0, True)
    for s in range(1, planes):
        collect(s, False)

    def closing(t, z):
        r = pl.ds(pl.multiple_of(t * TILE, TILE), TILE)
        moe_out[r, :] = rms_scale(comb[r, :], trail[...]).astype(bf)
        return z

    lax.fori_loop(0, TOK_DEV // TILE, closing, 0)
    last = pltpu.make_async_copy(moe_out, moe_hbm_out, moe_sem)
    last.start()

    def finish(s, z):
        k = (i + s) % n
        over_c(k).wait_send()
        over_d(k).wait_send()
        home(k).wait_send()
        return z

    lax.fori_loop(1, n, finish, 0)

    def finish_far(s, z):
        q = plane(s)

        @pl.when(s < planes - 1)
        def _():
            over_x(q * group + g).wait_send()

        @pl.when(s <= early)
        def _():
            for r in range(1, group):
                over_x(q * group + (g + r) % group).wait_send()

        @pl.when(direct(s))
        def _():
            for r in range(1, group):
                over_xy(q, r).wait_send()

        for r in range(1, group):
            over_y(q, r).wait_send()

        @pl.when((q < p) & (p + 1 < planes))
        def _():
            for copy in step_right(q, relay.at[q], meta.at[q]):
                copy.wait_send()

        @pl.when((q > p) & (p >= 1))
        def _():
            for copy in step_left(q, relay.at[q], meta.at[q]):
                copy.wait_send()

        return z

    lax.fori_loop(1, planes, finish_far, 0)

    @pl.when(p + 1 < planes)
    def _():
        for copy in step_right(p, nt.at[j], rk.at[j]):
            copy.wait_send()
        chain().wait_send()

    @pl.when(p >= 1)
    def _():
        for copy in step_left(p, nt.at[j], rk.at[j]):
            copy.wait_send()

    if planes > 1:
        for side in range(2):

            @pl.when((p < planes - 1) if side == 0 else (p > 0))
            def _():
                for copy in twin(side, False):
                    copy.wait_send()

        for r in range(1, group):
            twin_y(r).wait_send()
    for r in range(1, group):
        for w in range(2):
            near(r, w).wait_send()
        for copy in in_plane(r):
            copy.wait_send()
    for c in range(PIECES):
        store(c).wait()
    last.wait()


def shards(
    state_probe_logits,
    retention_logits,
    state_source_entries,
    state_result_switch_logits,
    retention_bound_margin,
    extra_fading_amount,
    state_result_scale,
    state_result_matrix,
    second_slice_tokens,
    specialist_assignment,
    selected_specialist_share,
    leading_scale_vector,
    trailing_scale_vector,
    specialist_switch_matrix,
    specialist_widen_matrix,
    specialist_contract_matrix,
):
    n = lax.axis_size("ep")
    experts = specialist_switch_matrix.shape[0] * n
    top_count = specialist_assignment.shape[1]
    capacity = 2 * TOK_DEV * top_count // experts
    planes = STAGES if n % (2 * STAGES) == 0 else 1
    group = n // planes
    length, width = state_probe_logits.shape
    heads = width // HEAD
    features = second_slice_tokens.shape[1]
    hidden = specialist_switch_matrix.shape[2]
    columns = state_result_matrix.shape[1]
    bf, f32 = jnp.bfloat16, jnp.float32
    hbm = pl.BlockSpec(memory_space=pltpu.HBM)
    chunk = (capacity, features)
    block = (TOK_DEV, features)
    return tuple(
        pl.pallas_call(
            functools.partial(kernel, n, planes, capacity, experts),
            name="fused",
            out_shape=(
                jax.ShapeDtypeStruct((length, columns), bf),
                jax.ShapeDtypeStruct(block, bf),
            ),
            in_specs=[hbm] * 16,
            out_specs=(hbm, hbm),
            scratch_shapes=[
                VMEM((length, columns), bf),
                VMEM(block, bf),
                VMEM((top_count, 4 * TOK_DEV), jnp.int32),
                VMEM((top_count, 4 * TOK_DEV), f32),
                VMEM((1, width), f32),
                VMEM((heads, length), f32),
                VMEM((1, width), f32),
                VMEM((1, features), f32),
                VMEM((1, features), f32),
                VMEM((4,) + block, bf),
                VMEM((length, width), bf),
                VMEM((length, width), bf),
                VMEM((length, width), bf),
                VMEM((length, width), bf),
                VMEM(state_result_matrix.shape, bf),
                VMEM((features, hidden), bf),
                VMEM((features, hidden), bf),
                VMEM((hidden, features), bf),
                VMEM((4, experts, TOK_DEV), f32),
                VMEM((4, experts, TOK_DEV), f32),
                VMEM((planes, experts, TOK_DEV), f32),
                VMEM((planes,) + block, bf),
                VMEM((2, experts, TOK_DEV), f32),
                VMEM((2,) + block, bf),
                VMEM((n, 4) + chunk, bf),
                VMEM((n, 4) + chunk, bf),
                VMEM((2, n) + chunk, bf),
                VMEM((n,) + chunk, bf),
                VMEM((n,) + chunk, bf),
                VMEM((n,) + chunk, bf),
                VMEM((planes, group - 1) + chunk, bf),
                VMEM((group - 1,) + chunk, bf),
                VMEM((2, group - 1) + chunk, bf),
                VMEM(block, f32),
                VMEM((n * capacity, TOK_DEV), f32),
                VMEM((planes, TOK_DEV, TOK_DEV), bf),
                VMEM((planes, TOK_DEV, TOK_DEV), bf),
                VMEM((length, width), f32),
                VMEM((length, width), bf),
                VMEM((heads, HEAD, HEAD), f32),
                VMEM((heads, HEAD, HEAD), bf),
                VMEM((8, width), f32),
                VMEM((group, heads, HEAD, HEAD), bf),
                VMEM((group, 8, width), f32),
                VMEM((heads, HEAD, HEAD), bf),
                VMEM((heads, HEAD, HEAD), bf),
                VMEM((heads, HEAD, HEAD), f32),
                VMEM((heads, HEAD, HEAD), f32),
                VMEM((4, length, width), bf),
                DMA((16,)), DMA((PIECES,)), DMA,
                DMA((2, planes)), DMA((planes,)), DMA((2, planes)), DMA((planes,)),
                DMA((planes, group)), DMA((n,)), DMA((2, group)), DMA((2, n)),
                DMA((2, 2)), DMA((2, 2)), DMA((group,)), DMA((n,)),
                DMA((planes, group)), DMA((n,)),
            ]
            + [DMA((n,))] * 14
            + [DMA((group,))] * 4
            + [DMA, DMA]
            + [DMA((PIECES,))] * 6,
            compiler_params=pltpu.CompilerParams(
                collective_id=0, has_side_effects=True, vmem_limit_bytes=LIMIT * 2**20
            ),
        )(
            specialist_assignment.T,
            selected_specialist_share.T,
            retention_bound_margin[None, :],
            extra_fading_amount.T,
            state_result_scale[None, :],
            leading_scale_vector[None, :],
            trailing_scale_vector[None, :],
            second_slice_tokens.reshape((4,) + block),
            state_probe_logits,
            retention_logits,
            state_source_entries,
            state_result_switch_logits,
            state_result_matrix,
            specialist_switch_matrix[0],
            specialist_widen_matrix[0],
            specialist_contract_matrix[0],
        )
    )


def solution(mesh):
    return jax.shard_map(
        shards,
        mesh=mesh,
        in_specs=(
            P("ep", "tp"),
            P("ep", "tp"),
            P("ep", "tp"),
            P("ep", "tp"),
            P("tp"),
            P("ep", "tp"),
            P("tp"),
            P(None, "tp"),
            P("ep", None),
            P("ep", None),
            P("ep", None),
            P(),
            P(),
            P("ep", None, "tp"),
            P("ep", None, "tp"),
            P("ep", "tp", None),
        ),
        out_specs=(P("ep", "tp"), P(("ep", "tp"), None)),
        check_vma=False,
    )
```

```python
import functools

import jax
import jax.numpy as jnp
from jax import lax
from jax.experimental import pallas as pl
from jax.experimental.pallas import tpu as pltpu
from jax.sharding import PartitionSpec as P

HEAD = 128
SPAN = 128
TOK_DEV = 128
STAGES = 4
PIECES = 4
STEP = 512
TILE = 16
LIMIT = 62

NORM_EPS = 1e-06
SWISH_ALPHA = 1.702
CLAMP_LIMIT = 7.0
MESH = pl.DeviceIdType.MESH
VMEM = pltpu.VMEM
DMA = pltpu.SemaphoreType.DMA
NT = (((1,), (1,)), ((), ()))
TN = (((0,), (0,)), ((), ()))


def remote(src, dst, send, recv, where):
    return pltpu.make_async_remote_copy(
        src_ref=src, dst_ref=dst, send_sem=send, recv_sem=recv, device_id=where, device_id_type=MESH
    )


def clamped_unit(gate, upward):
    glued = jnp.minimum(gate, CLAMP_LIMIT)
    linear = jnp.clip(upward, -CLAMP_LIMIT, CLAMP_LIMIT)
    return glued * jax.nn.sigmoid(SWISH_ALPHA * glued) * (linear + 1.0)


def rms_scale(values, gain):
    return values * lax.rsqrt(jnp.mean(values * values, axis=-1, keepdims=True) + NORM_EPS) * gain


def span_step(t, probe, ret, val, margin, extra, raw, qdec, state, running):
    rows = pl.ds(pl.multiple_of(t * SPAN, SPAN), SPAN)
    width = probe.shape[1]
    x = probe[rows, :].astype(jnp.float32)
    q = x * jax.nn.sigmoid(x) * HEAD ** (-0.5)
    k = margin[...] * jax.nn.sigmoid(-ret[rows, :].astype(jnp.float32))
    logs = jnp.log1p(-k)
    row = lax.broadcasted_iota(jnp.int32, (SPAN, SPAN), 0)
    col = lax.broadcasted_iota(jnp.int32, (SPAN, SPAN), 1)
    causal = row >= col
    tril = jnp.where(causal, 1.0, 0.0).astype(jnp.float32)
    for h in range(width // HEAD):
        cols = slice(h * HEAD, (h + 1) * HEAD)
        qh, kh = q[:, cols], k[:, cols]
        fade = jnp.transpose(jnp.broadcast_to(extra[h : h + 1, rows], (SPAN, SPAN)))
        ld = logs[:, cols] + fade
        cum = jnp.dot(
            tril, ld, precision=lax.Precision.HIGHEST, preferred_element_type=jnp.float32
        )
        middle = cum[SPAN // 2 - 1 : SPAN // 2, :]
        last = cum[SPAN - 1 :, :]
        a = (qh * jnp.exp(cum - middle)).astype(jnp.bfloat16)
        b = (kh * jnp.exp(middle - cum)).astype(jnp.bfloat16)
        qe = qh * jnp.exp(cum)
        kd = (kh * jnp.exp(last - cum)).astype(jnp.bfloat16)
        v = val[rows, cols]
        s = lax.dot_general(a, b, NT, preferred_element_type=jnp.float32)
        s = jnp.where(causal, s, 0.0).astype(jnp.bfloat16)
        st = state[h]
        out = jnp.dot(s, v, preferred_element_type=jnp.float32)
        out = out + lax.dot_general(
            qe.astype(jnp.bfloat16), st.astype(jnp.bfloat16), NT, preferred_element_type=jnp.float32
        )
        raw[rows, cols] = out
        before = running[0:1, cols]
        qdec[rows, cols] = (qe * jnp.exp(before)).astype(jnp.bfloat16)
        state[h] = jnp.exp(last) * st + lax.dot_general(
            v, kd, TN, preferred_element_type=jnp.float32
        )
        running[:, cols] = running[:, cols] + last


def kernel(
    n, planes, capacity, experts,
    named_hbm, shared_hbm, margin_hbm, extra_hbm, scale_hbm, lead_hbm, trail_hbm, tok_hbm, probe_hbm, ret_hbm, val_hbm, switch_hbm, mix_hbm, gate_hbm, up_hbm, down_hbm,
    mix_hbm_out, moe_hbm_out,
    mix_out, moe_out,
    named_by, shared_by, margin, extra, scale, lead, trail, nt, probe, ret, val, switch, mix_w, gate_w, up_w, down_w,
    act, rk, sh, meta, relay, meta2, relay2, rows, part, acc, sendb, recvb, back, pk, pk2, pko, comb, spread, share_hi, share_lo,
    raw, qdec, state, state_bf, running, plst, pld, chain_in, chain_out, enter, carry, gath,
    load_sem, store_sem, moe_sem,
    fsend, frecv, msend, mrecv, ysend, yrecv, zsend, zrecv, tsend, trecv, vsend, vrecv, qsend, qrecv,
    xsend, xrecv, csend, crecv, dsend, drecv,
    esend0, erecv0, esend1, erecv1, bsend, brecv, rsend, rrecv,
    pssend, psrecv, pdsend, pdrecv, chsend, chrecv,
    gxsend, gxrecv, gcsend, gcrecv, gdsend, gdrecv,
):
    i, j = lax.axis_index("ep"), lax.axis_index("tp")
    mate = j + 1 - 2 * (j % 2)
    cross = (j + 2) % 4
    mate_cross = (mate + 2) % 4
    group = n // planes
    p, g = i // group, i % group
    features = nt.shape[2]
    heads = state.shape[0]
    width = probe.shape[1]
    length = probe.shape[0]
    f32, bf = jnp.float32, jnp.bfloat16

    pairs = (
        (tok_hbm, nt), (lead_hbm, lead), (named_hbm, named_by), (shared_hbm, shared_by),
        (margin_hbm, margin), (extra_hbm, extra),
        (probe_hbm, probe), (ret_hbm, ret), (val_hbm, val),
        (gate_hbm, gate_w), (up_hbm, up_w), (down_hbm, down_w),
        (switch_hbm, switch), (mix_hbm, mix_w), (scale_hbm, scale), (trail_hbm, trail),
    )
    loads = [pltpu.make_async_copy(a, b, load_sem.at[w]) for w, (a, b) in enumerate(pairs)]
    for load in loads:
        load.start()

    barrier = pltpu.get_barrier_semaphore()

    def hello(s, c):
        pl.semaphore_signal(barrier, inc=1, device_id=((i + s) % n, j), device_id_type=MESH)
        return c

    lax.fori_loop(1, n, hello, 0)
    for t in (mate, cross):
        pl.semaphore_signal(barrier, inc=1, device_id=(i, t), device_id_type=MESH)
    for r in range(1, group):
        d = p * group + (g + r) % group
        pl.semaphore_signal(barrier, inc=1, device_id=(d, cross), device_id_type=MESH)

    more = (p + planes - 1) // planes
    less = (2 * planes - 2 - p) // planes
    early = more * less

    def plane(s):
        left, right = p, planes - 1 - p
        big = (left - right + planes) // planes
        small = big * right + (1 - big) * left
        t = s - 1 + 2 * planes
        both = 1 - (t - 2 * small) // (2 * planes)
        t = t - 2 * planes
        far = both * ((t + 2) // 2) + (1 - both) * (s - small)
        sign = (2 * big - 1) * (2 * both * (s % 2) - 1)
        other = (s + planes - 1) // planes - s // planes
        return p + other * sign * far

    half = max(group // 2, 1)

    def table(h, values):
        total = values[0]
        for v in range(1, len(values)):
            total = total + (values[v] - values[v - 1]) * ((h + len(values) - v) // len(values))
        return total

    def place(c):
        away = (c + 1 - group + n) // n
        rest = away * (c + 1 - group)
        h = rest // half
        inside = (table(h, (2, 2, 3, 3, 1, 1)), table(h, (0, 0, 2, 2, 4, 4)))
        outside = (table(h, (2, 2, 1, 3, 3, 1)), table(h, (0, 0, 2, 3, 3, 4)))
        s, base = (early * a + (1 - early) * b for a, b in zip(inside, outside))
        s = away * s
        r = away * (rest - half * base) + (1 - away) * (c + 1)
        q = plane(s)
        return s, r, q * group + (g + r) % group

    def ranks():
        ids = lax.broadcasted_iota(jnp.int32, (experts, TOK_DEV), 0)
        one = lax.broadcasted_iota(jnp.int32, (TOK_DEV, TOK_DEV), 0)
        two = lax.broadcasted_iota(jnp.int32, (TOK_DEV, TOK_DEV), 1)
        earlier = jnp.where(one < two, 1.0, 0.0).astype(bf)
        top = named_by.shape[0]
        for b in range(4):
            lanes = slice(b * TOK_DEV, (b + 1) * TOK_DEV)
            named = jnp.zeros((experts, TOK_DEV), f32)
            share = jnp.zeros((experts, TOK_DEV), f32)
            for w in range(top):
                hit = ids == named_by[w : w + 1, lanes]
                named = named + jnp.where(hit, 1.0, 0.0)
                share = share + jnp.where(hit, shared_by[w : w + 1, lanes], 0.0)
            ahead = jnp.dot(named.astype(bf), earlier, preferred_element_type=f32)
            rk[b] = jnp.where(named > 0.5, ahead, -1.0)
            sh[b] = share

    def norm(b):
        def tile(t, c):
            r = pl.ds(pl.multiple_of(t * TILE, TILE), TILE)
            nt[b, r, :] = rms_scale(nt[b, r, :].astype(f32), lead[...]).astype(bf)
            return c

        lax.fori_loop(0, TOK_DEV // TILE, tile, 0)

    slot = lax.broadcasted_iota(jnp.int32, (capacity, TOK_DEV), 0).astype(f32)

    def one_hot(ranked, e):
        return jnp.where(slot == ranked[pl.ds(e, 1), :], 1.0, 0.0)

    def pack(ranked, tokens, own, others):
        picks = [one_hot(ranked, i)]
        if others is not None:
            picks += [one_hot(ranked, p * group + (g + r) % group) for r in range(1, group)]
        pick = (picks[0] if len(picks) == 1 else jnp.concatenate(picks, axis=0)).astype(bf)
        for f in range(0, features, STEP):
            y = jnp.dot(pick, tokens[:, f : f + STEP], preferred_element_type=f32).astype(bf)
            own[:, f : f + STEP] = y[:capacity]
            for r in range(1, len(picks)):
                others[r - 1, :, f : f + STEP] = y[r * capacity : (r + 1) * capacity]

    def step_right(q, src, info):
        return (
            remote(src, relay.at[q], fsend.at[0, q], frecv.at[q], (i + group, j)),
            remote(info, meta.at[q], msend.at[0, q], mrecv.at[q], (i + group, j)),
        )

    def step_left(q, src, info):
        return (
            remote(src, relay.at[q], fsend.at[1, q], frecv.at[q], (i - group, j)),
            remote(info, meta.at[q], msend.at[1, q], mrecv.at[q], (i - group, j)),
        )

    def over_y(q, r):
        k = q * group + g
        d = p * group + (g + r) % group
        return remote(pk.at[q, r - 1], rows.at[k, j], ysend.at[q, r], yrecv.at[k], (d, j))

    def got_y(k):
        return remote(pk.at[0, 0], rows.at[k, j], ysend.at[0, 0], yrecv.at[k], (i, mate))

    def over_xy(q, r):
        k = q * group + g
        d = p * group + (g + r) % group
        return remote(pk.at[q, r - 1], rows.at[k, j], qsend.at[q, r], qrecv.at[k], (d, cross))

    def got_xy(k):
        return remote(pk.at[0, 0], rows.at[k, cross], qsend.at[0, 0], qrecv.at[k], (i, mate))

    def near(r, w):
        d = p * group + (g + r) % group
        b = (j, cross)[w]
        return remote(pko.at[w, r - 1], rows.at[i, b], zsend.at[w, r], zrecv.at[w, i], (d, j))

    def got_near(k, w):
        b = (j, cross)[w]
        return remote(pko.at[w, 0], rows.at[k, b], zsend.at[w, 0], zrecv.at[w, k], (i, mate))

    def over_x(k):
        return remote(rows.at[k, j], rows.at[k, j], xsend.at[k], xrecv.at[k], (i, cross))

    def over_c(k):
        return remote(rows.at[k, j], rows.at[k, j], csend.at[k], crecv.at[k], (i, mate))

    def over_d(k):
        return remote(rows.at[k, cross], rows.at[k, cross], dsend.at[k], drecv.at[k], (i, mate))

    def to_mate(k, close):
        if close:
            return remote(part.at[k, mate], acc.at[0, k], esend0.at[k], erecv0.at[k], (i, mate))
        return remote(
            part.at[k, mate_cross], acc.at[1, k], esend1.at[k], erecv1.at[k], (i, mate)
        )

    def to_cross(k):
        return remote(sendb.at[k], recvb.at[k], bsend.at[k], brecv.at[k], (i, cross))

    def home(k):
        return remote(sendb.at[k], back.at[i], rsend.at[k], rrecv.at[i], (k, j))

    def home_in(k):
        return remote(sendb.at[k], back.at[k], rsend.at[k], rrecv.at[k], (k, j))

    upper = 2 * p // planes
    source = (planes - 1) * (1 - upper)

    def twin(side, first):
        src = (nt.at[cross], rk.at[cross]) if first else (relay2.at[side], meta2.at[side])
        dst = (relay2.at[side], meta2.at[side])
        d = i + group - 2 * group * side
        return [
            remote(src[w], dst[w], tsend.at[side, w], trecv.at[side, w], (d, j)) for w in range(2)
        ]

    def twin_start():
        @pl.when(p == 0)
        def _():
            for copy in twin(0, True):
                copy.start()

        @pl.when(p == planes - 1)
        def _():
            for copy in twin(1, True):
                copy.start()

    def twin_pass(side, used):
        mine = (upper == 1) if side == 0 else (upper == 0)
        take = mine if used else jnp.logical_not(mine)
        reach = (p > 0) if side == 0 else (p < planes - 1)
        on = (p < planes - 1) if side == 0 else (p > 0)

        @pl.when(take & reach)
        def _():
            for copy in twin(side, False):
                copy.wait_recv()

        @pl.when(take & reach & on)
        def _():
            for copy in twin(side, False):
                copy.start()

    def twin_y(r):
        k = source * group + g
        d = p * group + (g + r) % group
        return remote(pk2.at[r - 1], rows.at[k, cross], vsend.at[r], vrecv.at[k], (d, j))

    def got_twin_y(k):
        return remote(pk2.at[0], rows.at[k, cross], vsend.at[0], vrecv.at[k], (i, mate))

    inner = (p >= 1) & (p + 1 < planes)

    def forward(s):
        q = plane(s)

        @pl.when(inner)
        def _():
            for copy in step_right(q, relay.at[q], meta.at[q]):
                copy.wait_recv()

        @pl.when(inner & (q < p))
        def _():
            for copy in step_right(q, relay.at[q], meta.at[q]):
                copy.start()

        @pl.when(inner & (q > p))
        def _():
            for copy in step_left(q, relay.at[q], meta.at[q]):
                copy.start()

    def direct(s):
        return (s >= 1) & (s < planes - 1) & (s > early)

    def late():
        over_x(plane(1) * group + g).start()

    def later():
        q = plane(1)
        for r in range(1, group):
            k = q * group + (g + r) % group
            got_y(k).wait_recv()
            over_x(k).start()

    def arrive(s):
        q = plane(s)
        k = q * group + g

        @pl.when((p == 0) | (p + 1 == planes))
        def _():
            for copy in step_right(q, relay.at[q], meta.at[q]):
                copy.wait_recv()

        pack(meta.at[q], relay.at[q], rows.at[k, j], pk.at[q])

        @pl.when(direct(s))
        def _():
            over_x(k).start()

        for r in range(1, group):
            over_y(q, r).start()

        @pl.when(direct(s))
        def _():
            for r in range(1, group):
                over_xy(q, r).start()

    def arrive_twin():
        k = source * group + g
        for side in range(2):
            twin_pass(side, True)
        for side in range(2):

            @pl.when(upper == 1 - side)
            def _():
                pack(meta2.at[side], relay2.at[side], rows.at[k, cross], pk2)

        for r in range(1, group):
            twin_y(r).start()

    def expert(k):
        x = rows[k].reshape(4 * capacity, features)
        gate = jnp.dot(x, gate_w[...], preferred_element_type=f32)
        upward = jnp.dot(x, up_w[...], preferred_element_type=f32)
        act[...] = clamped_unit(gate, upward).astype(bf).reshape(act.shape)
        for one, two in ((mate_cross, mate), (cross, j)):
            a = jnp.concatenate([act[one], act[two]], axis=0)
            for f in range(0, features, STEP):
                y = jnp.dot(a, down_w[:, f : f + STEP], preferred_element_type=f32).astype(bf)
                part[k, one, :, f : f + STEP] = y[:capacity]
                part[k, two, :, f : f + STEP] = y[capacity:]
            if one is mate_cross:
                to_mate(k, False).start()
                to_mate(k, True).start()

    def prepare(c):
        s, r, k = place(c)

        @pl.when(s == 0)
        def _():
            got_near(k, 0).wait_recv()
            got_near(k, 1).wait_recv()

        @pl.when((r >= 1) & (direct(s) | ((s >= 1) & (s == planes - 1))))
        def _():
            got_y(k).wait_recv()

        @pl.when((s >= 1) & (s == planes - 1) & (r >= 1))
        def _():
            got_twin_y(k).wait_recv()

        @pl.when(direct(s) & (r >= 1))
        def _():
            got_xy(k).wait_recv()

        @pl.when((s >= 1) & (s < planes - 1) & ((r == 0) | (s <= early)))
        def _():
            over_x(k).wait_recv()

        over_c(k).start()
        over_d(k).start()

    def work(k):
        over_c(k).wait_recv()
        over_d(k).wait_recv()
        expert(k)

    def first_sum(k):
        to_mate(k, False).wait()
        x = part[k, cross].astype(f32) + acc[1, k].astype(f32)
        sendb[k] = x.astype(bf)

    def total(k):
        to_mate(k, True).wait()
        to_cross(k).wait()
        x = part[k, j].astype(f32) + acc[0, k].astype(f32)
        return (x + recvb[k].astype(f32)).astype(bf)

    def in_plane(r):
        d = p * group + (g + r) % group
        return (
            remote(state_bf, plst.at[g], pssend.at[r], psrecv.at[g], (d, j)),
            remote(running, pld.at[g], pdsend.at[r], pdrecv.at[g], (d, j)),
        )

    def in_plane_got(r):
        o = (g + r) % group
        return (
            remote(state_bf, plst.at[o], pssend.at[r], psrecv.at[o], (i, mate)),
            remote(running, pld.at[o], pdsend.at[r], pdrecv.at[o], (i, mate)),
        )

    def chain():
        return remote(chain_out, chain_in, chsend, chrecv, (i + group, j))

    def prefix():
        for r in range(1, group):
            for copy in in_plane_got(r):
                copy.wait_recv()

        @pl.when(p == 0)
        def _():
            carry[...] = jnp.zeros_like(carry)

        @pl.when(p >= 1)
        def _():
            chain().wait_recv()
            carry[...] = chain_in[...].astype(f32)

        for o in range(group):
            @pl.when(g == o)
            def _():
                enter[...] = carry[...]

            for h in range(heads):
                d = pld[o, 0:1, h * HEAD : (h + 1) * HEAD]
                carry[h] = jnp.exp(d) * carry[h] + plst[o, h].astype(f32)

        @pl.when(p + 1 < planes)
        def _():
            chain_out[...] = carry[...].astype(bf)
            chain().start()

    piece = length // PIECES

    def at(c):
        return pl.ds(pl.multiple_of(c * piece, piece), piece)

    def mix_x(c):
        here = gath.at[j, at(c)]
        return remote(here, here, gxsend.at[c], gxrecv.at[c], (i, cross))

    def mix_c(c):
        here = gath.at[j, at(c)]
        return remote(here, here, gcsend.at[c], gcrecv.at[c], (i, mate))

    def mix_d(c):
        here = gath.at[cross, at(c)]
        return remote(here, here, gdsend.at[c], gdrecv.at[c], (i, mate))

    def store(c):
        return pltpu.make_async_copy(mix_out.at[at(c)], mix_hbm_out.at[at(c)], store_sem.at[c])

    def mix_final(c, z):
        r = at(c)
        for h in range(heads):
            cols = slice(h * HEAD, (h + 1) * HEAD)
            x = raw[r, cols] + lax.dot_general(
                qdec[r, cols], enter[h].astype(bf), NT, preferred_element_type=f32
            )
            x = x * lax.rsqrt(jnp.mean(x * x, axis=-1, keepdims=True) + NORM_EPS)
            v = switch[r, cols].astype(f32)
            gath[j, r, cols] = (x * scale[:, cols] * (v * jax.nn.sigmoid(v))).astype(bf)
        mix_x(c).start()
        mix_c(c).start()
        return z

    def mix_pass(c, z):
        mix_x(c).wait()
        mix_d(c).start()
        return z

    def mix_project(c, z):
        mix_c(c).wait()
        mix_d(c).wait()
        r = at(c)
        a = jnp.dot(gath[0, r, :], mix_w[0:width, :], preferred_element_type=f32)
        for w in range(1, 4):
            a = a + jnp.dot(
                gath[w, r, :], mix_w[w * width : (w + 1) * width, :], preferred_element_type=f32
            )
        mix_out[r, :] = a.astype(bf)
        store(c).start()
        return z

    for load in loads[2:4]:
        load.wait()
    ranks()
    for load in loads[:2]:
        load.wait()
    norm(j)
    pl.semaphore_wait(barrier, n + group)

    @pl.when(p + 1 < planes)
    def _():
        for copy in step_right(p, nt.at[j], rk.at[j]):
            copy.start()

    @pl.when(p >= 1)
    def _():
        for copy in step_left(p, nt.at[j], rk.at[j]):
            copy.start()

    norm(cross)
    if planes > 1:
        twin_start()
    for w, b in enumerate((j, cross)):
        pack(rk.at[b], nt.at[b], rows.at[i, b], pko.at[w])
        for r in range(1, group):
            near(r, w).start()
    norm(mate)
    norm(mate_cross)
    for b in (mate, mate_cross):
        pack(rk.at[b], nt.at[b], rows.at[i, b], None)

    for load in loads[4:9]:
        load.wait()
    state[...] = jnp.zeros_like(state)
    running[...] = jnp.zeros_like(running)

    def spans(t, c):
        span_step(t, probe, ret, val, margin, extra, raw, qdec, state, running)
        return c

    for load in loads[9:]:
        load.wait()
    expert(i)
    first_sum(i)
    to_cross(i).start()
    lax.fori_loop(0, length // SPAN, spans, 0)
    for h in range(heads):
        state_bf[h] = state[h].astype(bf)
    plst[g] = state_bf[...]
    pld[g] = running[...]
    for r in range(1, group):
        for copy in in_plane(r):
            copy.start()
    for t in range(1, min(planes, 3)):
        forward(t)

    if planes > 1:
        @pl.when(early > 0)
        def _():
            arrive(2)

        arrive(1)
    prepare(0)

    def turn(u):
        return u - (1 - early) * ((u + n - group) // n)

    def busy(u):
        return (u >= 0) & (u < n - early) & ((early > 0) | (u != group - 1))

    def ready(u):
        @pl.when(busy(u))
        def _():
            prepare(turn(u))

    def pump(u, z):
        @pl.when((u >= 1) & (u < planes - 2))
        def _():
            forward(u + 2)

        @pl.when(u == 1)
        def _():
            for side in range(2):
                twin_pass(side, False)

        @pl.when(busy(u))
        def _():
            s, r, k = place(turn(u))
            work(k)
            first_sum(k)

            @pl.when((early > 0) | (u >= group))
            def _():
                to_cross(k).start()

        @pl.when((early == 0) & (u == group + 1))
        def _():
            for c in range(group - 1):
                s, r, k = place(c)
                to_cross(k).start()

        @pl.when(u == n - 1 - early)
        def _():
            lax.fori_loop(0, PIECES, mix_final, 0)

        if planes > 1:

            @pl.when((u == 1) | (u == 2 - early))
            def _():
                arrive(u + 1 + early)

            @pl.when((early > 0) & (u == 2))
            def _():
                late()

            @pl.when((early > 0) & (u == 3))
            def _():
                later()

        if planes > 1:

            @pl.when(u == 4 - 2 * early)
            def _():
                arrive_twin()

        @pl.when((u >= planes) & (early == 0))
        def _():
            ready(u + 1)

        @pl.when(busy(u - 1) & (u >= group + 1 - early))
        def _():
            s, r, k = place(turn(u - 1))
            sendb[k] = total(k)
            home(k).start()

        @pl.when(u == n - 2)
        def _():
            for c in range(group - 1):
                s, r, k = place(c)
                sendb[k] = total(k)
                home(k).start()

        @pl.when(u == 0)
        def _():
            back[i] = total(i)
            weights()

        @pl.when(u == p)
        def _():
            prefix()

        @pl.when((u < planes) | (early > 0))
        def _():
            ready(u + 1)

        return z

    def weights():
        lax.fori_loop(0, experts, weigh, 0)
        for b in range(n * capacity // TOK_DEV):
            wide = jnp.transpose(spread[b * TOK_DEV : (b + 1) * TOK_DEV, :])
            high = wide.astype(bf)
            share_hi[b] = high
            share_lo[b] = (wide - high.astype(f32)).astype(bf)

    def weigh(e, z):
        r = pl.ds(pl.multiple_of(e * capacity, capacity), capacity)
        spread[r, :] = jnp.where(
            slot == rk[j, pl.ds(e, 1), :], jnp.broadcast_to(sh[j, pl.ds(e, 1), :], slot.shape), 0.0
        )
        return z

    lax.fori_loop(0, n + 1, pump, 0)
    def mix_both(c, z):
        mix_pass(c, z)
        return mix_project(c - 1, z)

    mix_pass(0, 0)
    lax.fori_loop(1, PIECES, mix_both, 0)
    mix_project(PIECES - 1, 0)

    def finish(s, z):
        k = (i + s) % n
        over_c(k).wait_send()
        over_d(k).wait_send()
        return z

    lax.fori_loop(1, n, finish, 0)

    def finish_far(s, z):
        q = plane(s)

        @pl.when(s < planes - 1)
        def _():
            over_x(q * group + g).wait_send()

        @pl.when(s <= early)
        def _():
            for r in range(1, group):
                over_x(q * group + (g + r) % group).wait_send()

        @pl.when(direct(s))
        def _():
            for r in range(1, group):
                over_xy(q, r).wait_send()

        for r in range(1, group):
            over_y(q, r).wait_send()

        @pl.when((q < p) & (p + 1 < planes))
        def _():
            for copy in step_right(q, relay.at[q], meta.at[q]):
                copy.wait_send()

        @pl.when((q > p) & (p >= 1))
        def _():
            for copy in step_left(q, relay.at[q], meta.at[q]):
                copy.wait_send()

        return z

    lax.fori_loop(1, planes, finish_far, 0)

    @pl.when(p + 1 < planes)
    def _():
        for copy in step_right(p, nt.at[j], rk.at[j]):
            copy.wait_send()
        chain().wait_send()

    @pl.when(p >= 1)
    def _():
        for copy in step_left(p, nt.at[j], rk.at[j]):
            copy.wait_send()

    if planes > 1:
        for side in range(2):

            @pl.when((p < planes - 1) if side == 0 else (p > 0))
            def _():
                for copy in twin(side, False):
                    copy.wait_send()

        for r in range(1, group):
            twin_y(r).wait_send()
    for r in range(1, group):
        for w in range(2):
            near(r, w).wait_send()
        for copy in in_plane(r):
            copy.wait_send()
    def collect(s, first):
        q = plane(s)
        for r in range(group):
            k = q * group + (g + r) % group
            if s > 0 or r > 0:
                home_in(k).wait_recv()
        for f in range(0, features, STEP):
            flat = back[pl.ds(q * group, group), :, f : f + STEP].reshape(group * capacity, STEP)
            y = jnp.dot(share_hi[q], flat, preferred_element_type=f32) + jnp.dot(
                share_lo[q], flat, preferred_element_type=f32
            )
            comb[:, f : f + STEP] = y if first else comb[:, f : f + STEP] + y

    turns = [2, 3, 0, 1] if planes > 1 else [0]
    for s in turns:
        collect(s, s == turns[0])

    def closing(t, z):
        r = pl.ds(pl.multiple_of(t * TILE, TILE), TILE)
        moe_out[r, :] = rms_scale(comb[r, :], trail[...]).astype(bf)
        return z

    quarter = TOK_DEV // PIECES

    def last(c):
        r = pl.ds(pl.multiple_of(c * quarter, quarter), quarter)
        return pltpu.make_async_copy(moe_out.at[r], moe_hbm_out.at[r], moe_sem.at[c])

    def close(c, z):
        lax.fori_loop(c * (quarter // TILE), (c + 1) * (quarter // TILE), closing, 0)
        last(c).start()
        return z

    lax.fori_loop(0, PIECES, close, 0)

    def finish_home(s, z):
        home((i + s) % n).wait_send()
        return z

    lax.fori_loop(1, n, finish_home, 0)
    for c in range(PIECES):
        store(c).wait()
        last(c).wait()


def shards(
    state_probe_logits,
    retention_logits,
    state_source_entries,
    state_result_switch_logits,
    retention_bound_margin,
    extra_fading_amount,
    state_result_scale,
    state_result_matrix,
    second_slice_tokens,
    specialist_assignment,
    selected_specialist_share,
    leading_scale_vector,
    trailing_scale_vector,
    specialist_switch_matrix,
    specialist_widen_matrix,
    specialist_contract_matrix,
):
    n = lax.axis_size("ep")
    experts = specialist_switch_matrix.shape[0] * n
    top_count = specialist_assignment.shape[1]
    capacity = 2 * TOK_DEV * top_count // experts
    planes = STAGES if n % (2 * STAGES) == 0 else 1
    group = n // planes
    length, width = state_probe_logits.shape
    heads = width // HEAD
    features = second_slice_tokens.shape[1]
    hidden = specialist_switch_matrix.shape[2]
    columns = state_result_matrix.shape[1]
    bf, f32 = jnp.bfloat16, jnp.float32
    hbm = pl.BlockSpec(memory_space=pltpu.HBM)
    chunk = (capacity, features)
    block = (TOK_DEV, features)
    return tuple(
        pl.pallas_call(
            functools.partial(kernel, n, planes, capacity, experts),
            name="fused",
            out_shape=(
                jax.ShapeDtypeStruct((length, columns), bf),
                jax.ShapeDtypeStruct(block, bf),
            ),
            in_specs=[hbm] * 16,
            out_specs=(hbm, hbm),
            scratch_shapes=[
                VMEM((length, columns), bf),
                VMEM(block, bf),
                VMEM((top_count, 4 * TOK_DEV), jnp.int32),
                VMEM((top_count, 4 * TOK_DEV), f32),
                VMEM((1, width), f32),
                VMEM((heads, length), f32),
                VMEM((1, width), f32),
                VMEM((1, features), f32),
                VMEM((1, features), f32),
                VMEM((4,) + block, bf),
                VMEM((length, width), bf),
                VMEM((length, width), bf),
                VMEM((length, width), bf),
                VMEM((length, width), bf),
                VMEM(state_result_matrix.shape, bf),
                VMEM((features, hidden), bf),
                VMEM((features, hidden), bf),
                VMEM((hidden, features), bf),
                VMEM((4, capacity, hidden), bf),
                VMEM((4, experts, TOK_DEV), f32),
                VMEM((4, experts, TOK_DEV), f32),
                VMEM((planes, experts, TOK_DEV), f32),
                VMEM((planes,) + block, bf),
                VMEM((2, experts, TOK_DEV), f32),
                VMEM((2,) + block, bf),
                VMEM((n, 4) + chunk, bf),
                VMEM((n, 4) + chunk, bf),
                VMEM((2, n) + chunk, bf),
                VMEM((n,) + chunk, bf),
                VMEM((n,) + chunk, bf),
                VMEM((n,) + chunk, bf),
                VMEM((planes, group - 1) + chunk, bf),
                VMEM((group - 1,) + chunk, bf),
                VMEM((2, group - 1) + chunk, bf),
                VMEM(block, f32),
                VMEM((n * capacity, TOK_DEV), f32),
                VMEM((planes, TOK_DEV, TOK_DEV), bf),
                VMEM((planes, TOK_DEV, TOK_DEV), bf),
                VMEM((length, width), f32),
                VMEM((length, width), bf),
                VMEM((heads, HEAD, HEAD), f32),
                VMEM((heads, HEAD, HEAD), bf),
                VMEM((8, width), f32),
                VMEM((group, heads, HEAD, HEAD), bf),
                VMEM((group, 8, width), f32),
                VMEM((heads, HEAD, HEAD), bf),
                VMEM((heads, HEAD, HEAD), bf),
                VMEM((heads, HEAD, HEAD), f32),
                VMEM((heads, HEAD, HEAD), f32),
                VMEM((4, length, width), bf),
                DMA((16,)), DMA((PIECES,)), DMA((PIECES,)),
                DMA((2, planes)), DMA((planes,)), DMA((2, planes)), DMA((planes,)),
                DMA((planes, group)), DMA((n,)), DMA((2, group)), DMA((2, n)),
                DMA((2, 2)), DMA((2, 2)), DMA((group,)), DMA((n,)),
                DMA((planes, group)), DMA((n,)),
            ]
            + [DMA((n,))] * 14
            + [DMA((group,))] * 4
            + [DMA, DMA]
            + [DMA((PIECES,))] * 6,
            compiler_params=pltpu.CompilerParams(
                collective_id=0, has_side_effects=True, vmem_limit_bytes=LIMIT * 2**20
            ),
        )(
            specialist_assignment.T,
            selected_specialist_share.T,
            retention_bound_margin[None, :],
            extra_fading_amount.T,
            state_result_scale[None, :],
            leading_scale_vector[None, :],
            trailing_scale_vector[None, :],
            second_slice_tokens.reshape((4,) + block),
            state_probe_logits,
            retention_logits,
            state_source_entries,
            state_result_switch_logits,
            state_result_matrix,
            specialist_switch_matrix[0],
            specialist_widen_matrix[0],
            specialist_contract_matrix[0],
        )
    )


def solution(mesh):
    return jax.shard_map(
        shards,
        mesh=mesh,
        in_specs=(
            P("ep", "tp"),
            P("ep", "tp"),
            P("ep", "tp"),
            P("ep", "tp"),
            P("tp"),
            P("ep", "tp"),
            P("tp"),
            P(None, "tp"),
            P("ep", None),
            P("ep", None),
            P("ep", None),
            P(),
            P(),
            P("ep", None, "tp"),
            P("ep", None, "tp"),
            P("ep", "tp", None),
        ),
        out_specs=(P("ep", "tp"), P(("ep", "tp"), None)),
        check_vma=False,
    )
```

```python
import functools

import jax
import jax.numpy as jnp
from jax import lax
from jax.experimental import pallas as pl
from jax.experimental.pallas import tpu as pltpu
from jax.sharding import PartitionSpec as P

HEAD = 128
SPAN = 128
TOK_DEV = 128
STAGES = 4
PIECES = 4
STEP = 512
TILE = 16
LIMIT = 62

NORM_EPS = 1e-06
SWISH_ALPHA = 1.702
CLAMP_LIMIT = 7.0
MESH = pl.DeviceIdType.MESH
VMEM = pltpu.VMEM
DMA = pltpu.SemaphoreType.DMA
NT = (((1,), (1,)), ((), ()))
TN = (((0,), (0,)), ((), ()))


def remote(src, dst, send, recv, where):
    return pltpu.make_async_remote_copy(
        src_ref=src, dst_ref=dst, send_sem=send, recv_sem=recv, device_id=where, device_id_type=MESH
    )


def clamped_unit(gate, upward):
    glued = jnp.minimum(gate, CLAMP_LIMIT)
    linear = jnp.clip(upward, -CLAMP_LIMIT, CLAMP_LIMIT)
    return glued * jax.nn.sigmoid(SWISH_ALPHA * glued) * (linear + 1.0)


def rms_scale(values, gain):
    return values * lax.rsqrt(jnp.mean(values * values, axis=-1, keepdims=True) + NORM_EPS) * gain


def span_step(t, probe, ret, val, margin, extra, raw, qdec, state, running):
    rows = pl.ds(pl.multiple_of(t * SPAN, SPAN), SPAN)
    width = probe.shape[1]
    x = probe[rows, :].astype(jnp.float32)
    q = x * jax.nn.sigmoid(x) * HEAD ** (-0.5)
    k = margin[...] * jax.nn.sigmoid(-ret[rows, :].astype(jnp.float32))
    logs = jnp.log1p(-k)
    row = lax.broadcasted_iota(jnp.int32, (SPAN, SPAN), 0)
    col = lax.broadcasted_iota(jnp.int32, (SPAN, SPAN), 1)
    causal = row >= col
    tril = jnp.where(causal, 1.0, 0.0).astype(jnp.float32)
    for h in range(width // HEAD):
        cols = slice(h * HEAD, (h + 1) * HEAD)
        qh, kh = q[:, cols], k[:, cols]
        fade = jnp.transpose(jnp.broadcast_to(extra[h : h + 1, rows], (SPAN, SPAN)))
        ld = logs[:, cols] + fade
        cum = jnp.dot(
            tril, ld, precision=lax.Precision.HIGHEST, preferred_element_type=jnp.float32
        )
        middle = cum[SPAN // 2 - 1 : SPAN // 2, :]
        last = cum[SPAN - 1 :, :]
        a = (qh * jnp.exp(cum - middle)).astype(jnp.bfloat16)
        b = (kh * jnp.exp(middle - cum)).astype(jnp.bfloat16)
        qe = qh * jnp.exp(cum)
        kd = (kh * jnp.exp(last - cum)).astype(jnp.bfloat16)
        v = val[rows, cols]
        s = lax.dot_general(a, b, NT, preferred_element_type=jnp.float32)
        s = jnp.where(causal, s, 0.0).astype(jnp.bfloat16)
        st = state[h]
        out = jnp.dot(s, v, preferred_element_type=jnp.float32)
        out = out + lax.dot_general(
            qe.astype(jnp.bfloat16), st.astype(jnp.bfloat16), NT, preferred_element_type=jnp.float32
        )
        raw[rows, cols] = out
        before = running[0:1, cols]
        qdec[rows, cols] = (qe * jnp.exp(before)).astype(jnp.bfloat16)
        state[h] = jnp.exp(last) * st + lax.dot_general(
            v, kd, TN, preferred_element_type=jnp.float32
        )
        running[:, cols] = running[:, cols] + last


def kernel(
    n, planes, capacity, experts,
    named_hbm, shared_hbm, margin_hbm, extra_hbm, scale_hbm, lead_hbm, trail_hbm, tok_hbm, probe_hbm, ret_hbm, val_hbm, switch_hbm, mix_hbm, gate_hbm, up_hbm, down_hbm,
    mix_hbm_out, moe_hbm_out,
    mix_out, moe_out,
    named_by, shared_by, margin, extra, scale, lead, trail, nt, probe, ret, val, switch, mix_w, gate_w, up_w, down_w,
    act, rk, sh, meta, relay, meta2, relay2, rows, part, acc, sendb, recvb, back, pk, pk2, pko, comb, spread, share_hi, share_lo,
    raw, qdec, state, state_bf, running, plst, pld, chain_in, chain_out, enter, carry, gath,
    load_sem, store_sem, moe_sem,
    fsend, frecv, msend, mrecv, ysend, yrecv, zsend, zrecv, tsend, trecv, vsend, vrecv, qsend, qrecv,
    xsend, xrecv, csend, crecv, dsend, drecv,
    esend0, erecv0, esend1, erecv1, bsend, brecv, rsend, rrecv,
    pssend, psrecv, pdsend, pdrecv, chsend, chrecv,
    gxsend, gxrecv, gcsend, gcrecv, gdsend, gdrecv,
):
    i, j = lax.axis_index("ep"), lax.axis_index("tp")
    mate = j + 1 - 2 * (j % 2)
    cross = (j + 2) % 4
    mate_cross = (mate + 2) % 4
    group = n // planes
    p, g = i // group, i % group
    features = nt.shape[2]
    heads = state.shape[0]
    width = probe.shape[1]
    length = probe.shape[0]
    f32, bf = jnp.float32, jnp.bfloat16

    pairs = (
        (tok_hbm, nt), (lead_hbm, lead), (named_hbm, named_by), (shared_hbm, shared_by),
        (margin_hbm, margin), (extra_hbm, extra),
        (probe_hbm, probe), (ret_hbm, ret), (val_hbm, val),
        (gate_hbm, gate_w), (up_hbm, up_w), (down_hbm, down_w),
        (switch_hbm, switch), (mix_hbm, mix_w), (scale_hbm, scale), (trail_hbm, trail),
    )
    loads = [pltpu.make_async_copy(a, b, load_sem.at[w]) for w, (a, b) in enumerate(pairs)]
    for load in loads:
        load.start()

    barrier = pltpu.get_barrier_semaphore()

    def hello(s, c):
        pl.semaphore_signal(barrier, inc=1, device_id=((i + s) % n, j), device_id_type=MESH)
        return c

    lax.fori_loop(1, n, hello, 0)
    for t in (mate, cross):
        pl.semaphore_signal(barrier, inc=1, device_id=(i, t), device_id_type=MESH)
    for r in range(1, group):
        d = p * group + (g + r) % group
        pl.semaphore_signal(barrier, inc=1, device_id=(d, cross), device_id_type=MESH)

    more = (p + planes - 1) // planes
    less = (2 * planes - 2 - p) // planes
    early = more * less

    def plane(s):
        left, right = p, planes - 1 - p
        big = (left - right + planes) // planes
        small = big * right + (1 - big) * left
        t = s - 1 + 2 * planes
        both = 1 - (t - 2 * small) // (2 * planes)
        t = t - 2 * planes
        far = both * ((t + 2) // 2) + (1 - both) * (s - small)
        sign = (2 * big - 1) * (2 * both * (s % 2) - 1)
        other = (s + planes - 1) // planes - s // planes
        return p + other * sign * far

    half = max(group // 2, 1)

    def table(h, values):
        total = values[0]
        for v in range(1, len(values)):
            total = total + (values[v] - values[v - 1]) * ((h + len(values) - v) // len(values))
        return total

    def place(c):
        away = (c + 1 - group + n) // n
        rest = away * (c + 1 - group)
        h = rest // half
        inside = (table(h, (1, 1, 3, 3, 2, 2)), table(h, (0, 0, 2, 2, 4, 4)))
        outside = (table(h, (2, 2, 1, 3, 3, 1)), table(h, (0, 0, 2, 3, 3, 4)))
        s, base = (early * a + (1 - early) * b for a, b in zip(inside, outside))
        s = away * s
        r = away * (rest - half * base) + (1 - away) * (c + 1)
        q = plane(s)
        return s, r, q * group + (g + r) % group

    def ranks():
        ids = lax.broadcasted_iota(jnp.int32, (experts, TOK_DEV), 0)
        one = lax.broadcasted_iota(jnp.int32, (TOK_DEV, TOK_DEV), 0)
        two = lax.broadcasted_iota(jnp.int32, (TOK_DEV, TOK_DEV), 1)
        earlier = jnp.where(one < two, 1.0, 0.0).astype(bf)
        top = named_by.shape[0]
        for b in range(4):
            lanes = slice(b * TOK_DEV, (b + 1) * TOK_DEV)
            named = jnp.zeros((experts, TOK_DEV), f32)
            share = jnp.zeros((experts, TOK_DEV), f32)
            for w in range(top):
                hit = ids == named_by[w : w + 1, lanes]
                named = named + jnp.where(hit, 1.0, 0.0)
                share = share + jnp.where(hit, shared_by[w : w + 1, lanes], 0.0)
            ahead = jnp.dot(named.astype(bf), earlier, preferred_element_type=f32)
            rk[b] = jnp.where(named > 0.5, ahead, -1.0)
            sh[b] = share

    def norm(b):
        def tile(t, c):
            r = pl.ds(pl.multiple_of(t * TILE, TILE), TILE)
            nt[b, r, :] = rms_scale(nt[b, r, :].astype(f32), lead[...]).astype(bf)
            return c

        lax.fori_loop(0, TOK_DEV // TILE, tile, 0)

    slot = lax.broadcasted_iota(jnp.int32, (capacity, TOK_DEV), 0).astype(f32)

    def one_hot(ranked, e):
        return jnp.where(slot == ranked[pl.ds(e, 1), :], 1.0, 0.0)

    def pack(ranked, tokens, own, others):
        picks = [one_hot(ranked, i)]
        if others is not None:
            picks += [one_hot(ranked, p * group + (g + r) % group) for r in range(1, group)]
        pick = (picks[0] if len(picks) == 1 else jnp.concatenate(picks, axis=0)).astype(bf)
        for f in range(0, features, STEP):
            y = jnp.dot(pick, tokens[:, f : f + STEP], preferred_element_type=f32).astype(bf)
            own[:, f : f + STEP] = y[:capacity]
            for r in range(1, len(picks)):
                others[r - 1, :, f : f + STEP] = y[r * capacity : (r + 1) * capacity]

    part_rows = TOK_DEV // 2

    def step(q, src, info, side):
        d = i + group - 2 * group * side
        rows_of = [pl.ds(h * part_rows, part_rows) for h in range(2)]
        return [
            remote(info, meta.at[q], msend.at[side, q], mrecv.at[q], (d, j))
        ] + [
            remote(
                src.at[w], relay.at[q].at[w], fsend.at[side, q, h], frecv.at[q, h], (d, j)
            )
            for h, w in enumerate(rows_of)
        ]

    def step_right(q, src, info):
        return step(q, src, info, 0)

    def step_left(q, src, info):
        return step(q, src, info, 1)

    def over_y(q, r):
        k = q * group + g
        d = p * group + (g + r) % group
        return remote(pk.at[q, r - 1], rows.at[k, j], ysend.at[q, r], yrecv.at[k], (d, j))

    def got_y(k):
        return remote(pk.at[0, 0], rows.at[k, j], ysend.at[0, 0], yrecv.at[k], (i, mate))

    def over_xy(q, r):
        k = q * group + g
        d = p * group + (g + r) % group
        return remote(pk.at[q, r - 1], rows.at[k, j], qsend.at[q, r], qrecv.at[k], (d, cross))

    def got_xy(k):
        return remote(pk.at[0, 0], rows.at[k, cross], qsend.at[0, 0], qrecv.at[k], (i, mate))

    def near(r, w):
        d = p * group + (g + r) % group
        b = (j, cross)[w]
        return remote(pko.at[w, r - 1], rows.at[i, b], zsend.at[w, r], zrecv.at[w, i], (d, j))

    def got_near(k, w):
        b = (j, cross)[w]
        return remote(pko.at[w, 0], rows.at[k, b], zsend.at[w, 0], zrecv.at[w, k], (i, mate))

    def over_x(k):
        return remote(rows.at[k, j], rows.at[k, j], xsend.at[k], xrecv.at[k], (i, cross))

    def over_c(k):
        return remote(rows.at[k, j], rows.at[k, j], csend.at[k], crecv.at[k], (i, mate))

    def over_d(k):
        return remote(rows.at[k, cross], rows.at[k, cross], dsend.at[k], drecv.at[k], (i, mate))

    def to_mate(k, close):
        if close:
            return remote(part.at[k, mate], acc.at[0, k], esend0.at[k], erecv0.at[k], (i, mate))
        return remote(
            part.at[k, mate_cross], acc.at[1, k], esend1.at[k], erecv1.at[k], (i, mate)
        )

    def to_cross(k):
        return remote(sendb.at[k], recvb.at[k], bsend.at[k], brecv.at[k], (i, cross))

    def home(k):
        return remote(sendb.at[k], back.at[i], rsend.at[k], rrecv.at[i], (k, j))

    def home_in(k):
        return remote(sendb.at[k], back.at[k], rsend.at[k], rrecv.at[k], (k, j))

    upper = 2 * p // planes
    source = (planes - 1) * (1 - upper)

    def twin(side, first):
        src = (nt.at[cross], rk.at[cross]) if first else (relay2.at[side], meta2.at[side])
        dst = (relay2.at[side], meta2.at[side])
        d = i + group - 2 * group * side
        src, dst = (
            [v[1]] + [v[0].at[pl.ds(h * part_rows, part_rows)] for h in range(2)]
            for v in (src, dst)
        )
        return [
            remote(src[w], dst[w], tsend.at[side, w], trecv.at[side, w], (d, j)) for w in range(3)
        ]

    def twin_start():
        @pl.when(p == 0)
        def _():
            for copy in twin(0, True):
                copy.start()

        @pl.when(p == planes - 1)
        def _():
            for copy in twin(1, True):
                copy.start()

    def twin_pass(side, used):
        mine = (upper == 1) if side == 0 else (upper == 0)
        take = mine if used else jnp.logical_not(mine)
        reach = (p > 0) if side == 0 else (p < planes - 1)
        on = (p < planes - 1) if side == 0 else (p > 0)

        for which in (slice(0, 2), slice(2, 3)):

            @pl.when(take & reach)
            def _():
                for copy in twin(side, False)[which]:
                    copy.wait_recv()

            @pl.when(take & reach & on)
            def _():
                for copy in twin(side, False)[which]:
                    copy.start()

    def twin_y(r):
        k = source * group + g
        d = p * group + (g + r) % group
        return remote(pk2.at[r - 1], rows.at[k, cross], vsend.at[r], vrecv.at[k], (d, j))

    def got_twin_y(k):
        return remote(pk2.at[0], rows.at[k, cross], vsend.at[0], vrecv.at[k], (i, mate))

    inner = (p >= 1) & (p + 1 < planes)

    def forward(s, h):
        q = plane(s)
        which = slice(0, 2) if h == 0 else slice(2, 3)

        @pl.when(inner)
        def _():
            for copy in step_right(q, relay.at[q], meta.at[q])[which]:
                copy.wait_recv()

        @pl.when(inner & (q < p))
        def _():
            for copy in step_right(q, relay.at[q], meta.at[q])[which]:
                copy.start()

        @pl.when(inner & (q > p))
        def _():
            for copy in step_left(q, relay.at[q], meta.at[q])[which]:
                copy.start()

    def direct(s):
        return (s >= 1) & (s < planes - 1) & (s != 2 * early)

    def late():
        over_x(plane(2) * group + g).start()

    def later():
        q = plane(2)
        for r in range(1, group):
            k = q * group + (g + r) % group
            got_y(k).wait_recv()
            over_x(k).start()

    def arrive(s):
        q = plane(s)
        k = q * group + g

        @pl.when((p == 0) | (p + 1 == planes))
        def _():
            for copy in step_right(q, relay.at[q], meta.at[q]):
                copy.wait_recv()

        pack(meta.at[q], relay.at[q], rows.at[k, j], pk.at[q])

        @pl.when(direct(s))
        def _():
            over_x(k).start()

        for r in range(1, group):
            over_y(q, r).start()

        @pl.when(direct(s))
        def _():
            for r in range(1, group):
                over_xy(q, r).start()

    def arrive_twin():
        k = source * group + g
        for side in range(2):
            twin_pass(side, True)
        for side in range(2):

            @pl.when(upper == 1 - side)
            def _():
                pack(meta2.at[side], relay2.at[side], rows.at[k, cross], pk2)

        for r in range(1, group):
            twin_y(r).start()

    def expert(k):
        x = rows[k].reshape(4 * capacity, features)
        gate = jnp.dot(x, gate_w[...], preferred_element_type=f32)
        upward = jnp.dot(x, up_w[...], preferred_element_type=f32)
        act[...] = clamped_unit(gate, upward).astype(bf).reshape(act.shape)
        for one, two in ((mate_cross, mate), (cross, j)):
            a = jnp.concatenate([act[one], act[two]], axis=0)
            for f in range(0, features, STEP):
                y = jnp.dot(a, down_w[:, f : f + STEP], preferred_element_type=f32).astype(bf)
                part[k, one, :, f : f + STEP] = y[:capacity]
                part[k, two, :, f : f + STEP] = y[capacity:]
            if one is mate_cross:
                to_mate(k, False).start()
                to_mate(k, True).start()

    def prepare(c):
        s, r, k = place(c)

        @pl.when(s == 0)
        def _():
            got_near(k, 0).wait_recv()
            got_near(k, 1).wait_recv()

        @pl.when((r >= 1) & (direct(s) | ((s >= 1) & (s == planes - 1))))
        def _():
            got_y(k).wait_recv()

        @pl.when((s >= 1) & (s == planes - 1) & (r >= 1))
        def _():
            got_twin_y(k).wait_recv()

        @pl.when(direct(s) & (r >= 1))
        def _():
            got_xy(k).wait_recv()

        @pl.when((s >= 1) & (s < planes - 1) & ((r == 0) | (s == 2 * early)))
        def _():
            over_x(k).wait_recv()

        over_c(k).start()
        over_d(k).start()

    def work(k):
        over_c(k).wait_recv()
        over_d(k).wait_recv()
        expert(k)

    def first_sum(k):
        to_mate(k, False).wait()
        x = part[k, cross].astype(f32) + acc[1, k].astype(f32)
        sendb[k] = x.astype(bf)

    def total(k):
        to_mate(k, True).wait()
        to_cross(k).wait()
        x = part[k, j].astype(f32) + acc[0, k].astype(f32)
        return (x + recvb[k].astype(f32)).astype(bf)

    def in_plane(r):
        d = p * group + (g + r) % group
        return (
            remote(state_bf, plst.at[g], pssend.at[r], psrecv.at[g], (d, j)),
            remote(running, pld.at[g], pdsend.at[r], pdrecv.at[g], (d, j)),
        )

    def in_plane_got(r):
        o = (g + r) % group
        return (
            remote(state_bf, plst.at[o], pssend.at[r], psrecv.at[o], (i, mate)),
            remote(running, pld.at[o], pdsend.at[r], pdrecv.at[o], (i, mate)),
        )

    def chain():
        return remote(chain_out, chain_in, chsend, chrecv, (i + group, j))

    def prefix():
        for r in range(1, group):
            for copy in in_plane_got(r):
                copy.wait_recv()

        @pl.when(p == 0)
        def _():
            carry[...] = jnp.zeros_like(carry)

        @pl.when(p >= 1)
        def _():
            chain().wait_recv()
            carry[...] = chain_in[...].astype(f32)

        for o in range(group):
            @pl.when(g == o)
            def _():
                enter[...] = carry[...]

            for h in range(heads):
                d = pld[o, 0:1, h * HEAD : (h + 1) * HEAD]
                carry[h] = jnp.exp(d) * carry[h] + plst[o, h].astype(f32)

        @pl.when(p + 1 < planes)
        def _():
            chain_out[...] = carry[...].astype(bf)
            chain().start()

    piece = length // PIECES

    def at(c):
        return pl.ds(pl.multiple_of(c * piece, piece), piece)

    def mix_x(c):
        here = gath.at[j, at(c)]
        return remote(here, here, gxsend.at[c], gxrecv.at[c], (i, cross))

    def mix_c(c):
        here = gath.at[j, at(c)]
        return remote(here, here, gcsend.at[c], gcrecv.at[c], (i, mate))

    def mix_d(c):
        here = gath.at[cross, at(c)]
        return remote(here, here, gdsend.at[c], gdrecv.at[c], (i, mate))

    def store(c):
        return pltpu.make_async_copy(mix_out.at[at(c)], mix_hbm_out.at[at(c)], store_sem.at[c])

    def mix_final(c, z):
        r = at(c)
        for h in range(heads):
            cols = slice(h * HEAD, (h + 1) * HEAD)
            x = raw[r, cols] + lax.dot_general(
                qdec[r, cols], enter[h].astype(bf), NT, preferred_element_type=f32
            )
            x = x * lax.rsqrt(jnp.mean(x * x, axis=-1, keepdims=True) + NORM_EPS)
            v = switch[r, cols].astype(f32)
            gath[j, r, cols] = (x * scale[:, cols] * (v * jax.nn.sigmoid(v))).astype(bf)
        mix_x(c).start()
        mix_c(c).start()
        return z

    def mix_pass(c, z):
        mix_x(c).wait()
        mix_d(c).start()
        return z

    def mix_project(c, z):
        mix_c(c).wait()
        mix_d(c).wait()
        r = at(c)
        a = jnp.dot(gath[0, r, :], mix_w[0:width, :], preferred_element_type=f32)
        for w in range(1, 4):
            a = a + jnp.dot(
                gath[w, r, :], mix_w[w * width : (w + 1) * width, :], preferred_element_type=f32
            )
        mix_out[r, :] = a.astype(bf)
        store(c).start()
        return z

    for load in loads[2:4]:
        load.wait()
    ranks()
    for load in loads[:2]:
        load.wait()
    norm(j)
    pl.semaphore_wait(barrier, n + group)

    @pl.when(p + 1 < planes)
    def _():
        for copy in step_right(p, nt.at[j], rk.at[j]):
            copy.start()

    @pl.when(p >= 1)
    def _():
        for copy in step_left(p, nt.at[j], rk.at[j]):
            copy.start()

    norm(cross)
    if planes > 1:
        twin_start()
    for w, b in enumerate((j, cross)):
        pack(rk.at[b], nt.at[b], rows.at[i, b], pko.at[w])
        for r in range(1, group):
            near(r, w).start()
    norm(mate)
    norm(mate_cross)
    for b in (mate, mate_cross):
        pack(rk.at[b], nt.at[b], rows.at[i, b], None)

    for load in loads[4:9]:
        load.wait()
    state[...] = jnp.zeros_like(state)
    running[...] = jnp.zeros_like(running)

    def spans(t, c):
        span_step(t, probe, ret, val, margin, extra, raw, qdec, state, running)
        return c

    for load in loads[9:]:
        load.wait()
    expert(i)
    first_sum(i)
    to_cross(i).start()
    lax.fori_loop(0, 2, spans, 0)
    for t in range(1, min(planes, 3)):
        forward(t, 0)
    lax.fori_loop(2, length // SPAN, spans, 0)
    for h in range(heads):
        state_bf[h] = state[h].astype(bf)
    plst[g] = state_bf[...]
    pld[g] = running[...]
    for r in range(1, group):
        for copy in in_plane(r):
            copy.start()
    for t in range(1, min(planes, 3)):
        forward(t, 1)

    if planes > 1:
        arrive(1)

        @pl.when(early > 0)
        def _():
            arrive(2)
    prepare(0)

    def turn(u):
        return u - (1 - early) * ((u + n - group) // n)

    def busy(u):
        return (u >= 0) & (u < n - early) & ((early > 0) | (u != group - 1))

    def ready(u):
        @pl.when(busy(u))
        def _():
            prepare(turn(u))

    def pump(u, z):
        @pl.when((u >= 1) & (u < planes - 2))
        def _():
            forward(u + 2, 1)

        @pl.when(u == 1)
        def _():
            for side in range(2):
                twin_pass(side, False)

        @pl.when(busy(u))
        def _():
            s, r, k = place(turn(u))
            work(k)
            first_sum(k)

            @pl.when((early > 0) | (u >= group))
            def _():
                to_cross(k).start()

        @pl.when((early == 0) & (u == group + 1))
        def _():
            for c in range(group - 1):
                s, r, k = place(c)
                to_cross(k).start()

        if planes > 1:

            @pl.when(u == 0)
            def _():
                forward(3, 0)

        @pl.when(u == n - 1 - early)
        def _():
            lax.fori_loop(0, PIECES, mix_final, 0)

        if planes > 1:

            @pl.when((u == 1) | (u == 2 - early))
            def _():
                arrive(u + 1 + early)

            @pl.when((early > 0) & (u == 2))
            def _():
                late()

            @pl.when((early > 0) & (u == 3))
            def _():
                later()

        if planes > 1:

            @pl.when(u == 3 - early)
            def _():
                arrive_twin()

        @pl.when((u >= planes) & (early == 0))
        def _():
            ready(u + 1)

        @pl.when(busy(u - 1) & (u >= group + 1 - early))
        def _():
            s, r, k = place(turn(u - 1))
            sendb[k] = total(k)
            home(k).start()

        @pl.when(u == n - 2)
        def _():
            for c in range(group - 1):
                s, r, k = place(c)
                sendb[k] = total(k)
                home(k).start()

        @pl.when(u == 0)
        def _():
            back[i] = total(i)
            weights()

        @pl.when(u == p)
        def _():
            prefix()

        @pl.when((u < planes) | (early > 0))
        def _():
            ready(u + 1)

        return z

    def weights():
        lax.fori_loop(0, experts, weigh, 0)
        for b in range(n * capacity // TOK_DEV):
            wide = jnp.transpose(spread[b * TOK_DEV : (b + 1) * TOK_DEV, :])
            high = wide.astype(bf)
            share_hi[b] = high
            share_lo[b] = (wide - high.astype(f32)).astype(bf)

    def weigh(e, z):
        r = pl.ds(pl.multiple_of(e * capacity, capacity), capacity)
        spread[r, :] = jnp.where(
            slot == rk[j, pl.ds(e, 1), :], jnp.broadcast_to(sh[j, pl.ds(e, 1), :], slot.shape), 0.0
        )
        return z

    lax.fori_loop(0, n + 1, pump, 0)
    def mix_both(c, z):
        mix_pass(c, z)
        return mix_project(c - 1, z)

    mix_pass(0, 0)
    lax.fori_loop(1, PIECES, mix_both, 0)
    mix_project(PIECES - 1, 0)

    def finish(s, z):
        k = (i + s) % n
        over_c(k).wait_send()
        over_d(k).wait_send()
        return z

    lax.fori_loop(1, n, finish, 0)

    def finish_far(s, z):
        q = plane(s)

        @pl.when(s < planes - 1)
        def _():
            over_x(q * group + g).wait_send()

        @pl.when(s == 2 * early)
        def _():
            for r in range(1, group):
                over_x(q * group + (g + r) % group).wait_send()

        @pl.when(direct(s))
        def _():
            for r in range(1, group):
                over_xy(q, r).wait_send()

        for r in range(1, group):
            over_y(q, r).wait_send()

        @pl.when((q < p) & (p + 1 < planes))
        def _():
            for copy in step_right(q, relay.at[q], meta.at[q]):
                copy.wait_send()

        @pl.when((q > p) & (p >= 1))
        def _():
            for copy in step_left(q, relay.at[q], meta.at[q]):
                copy.wait_send()

        return z

    lax.fori_loop(1, planes, finish_far, 0)

    @pl.when(p + 1 < planes)
    def _():
        for copy in step_right(p, nt.at[j], rk.at[j]):
            copy.wait_send()
        chain().wait_send()

    @pl.when(p >= 1)
    def _():
        for copy in step_left(p, nt.at[j], rk.at[j]):
            copy.wait_send()

    if planes > 1:
        for side in range(2):

            @pl.when((p < planes - 1) if side == 0 else (p > 0))
            def _():
                for copy in twin(side, False):
                    copy.wait_send()

        for r in range(1, group):
            twin_y(r).wait_send()
    for r in range(1, group):
        for w in range(2):
            near(r, w).wait_send()
        for copy in in_plane(r):
            copy.wait_send()
    def collect(s, first):
        q = plane(s)
        for r in range(group):
            k = q * group + (g + r) % group
            if s > 0 or r > 0:
                home_in(k).wait_recv()
        for f in range(0, features, STEP):
            flat = back[pl.ds(q * group, group), :, f : f + STEP].reshape(group * capacity, STEP)
            y = jnp.dot(share_hi[q], flat, preferred_element_type=f32) + jnp.dot(
                share_lo[q], flat, preferred_element_type=f32
            )
            comb[:, f : f + STEP] = y if first else comb[:, f : f + STEP] + y

    turns = [2, 3, 0, 1] if planes > 1 else [0]
    for s in turns:
        collect(s, s == turns[0])

    def closing(t, z):
        r = pl.ds(pl.multiple_of(t * TILE, TILE), TILE)
        moe_out[r, :] = rms_scale(comb[r, :], trail[...]).astype(bf)
        return z

    quarter = TOK_DEV // PIECES

    def last(c):
        r = pl.ds(pl.multiple_of(c * quarter, quarter), quarter)
        return pltpu.make_async_copy(moe_out.at[r], moe_hbm_out.at[r], moe_sem.at[c])

    def close(c, z):
        lax.fori_loop(c * (quarter // TILE), (c + 1) * (quarter // TILE), closing, 0)
        last(c).start()
        return z

    lax.fori_loop(0, PIECES, close, 0)

    def finish_home(s, z):
        home((i + s) % n).wait_send()
        return z

    lax.fori_loop(1, n, finish_home, 0)
    for c in range(PIECES):
        store(c).wait()
        last(c).wait()


def shards(
    state_probe_logits,
    retention_logits,
    state_source_entries,
    state_result_switch_logits,
    retention_bound_margin,
    extra_fading_amount,
    state_result_scale,
    state_result_matrix,
    second_slice_tokens,
    specialist_assignment,
    selected_specialist_share,
    leading_scale_vector,
    trailing_scale_vector,
    specialist_switch_matrix,
    specialist_widen_matrix,
    specialist_contract_matrix,
):
    n = lax.axis_size("ep")
    experts = specialist_switch_matrix.shape[0] * n
    top_count = specialist_assignment.shape[1]
    capacity = 2 * TOK_DEV * top_count // experts
    planes = STAGES if n % (2 * STAGES) == 0 else 1
    group = n // planes
    length, width = state_probe_logits.shape
    heads = width // HEAD
    features = second_slice_tokens.shape[1]
    hidden = specialist_switch_matrix.shape[2]
    columns = state_result_matrix.shape[1]
    bf, f32 = jnp.bfloat16, jnp.float32
    hbm = pl.BlockSpec(memory_space=pltpu.HBM)
    chunk = (capacity, features)
    block = (TOK_DEV, features)
    return tuple(
        pl.pallas_call(
            functools.partial(kernel, n, planes, capacity, experts),
            name="fused",
            out_shape=(
                jax.ShapeDtypeStruct((length, columns), bf),
                jax.ShapeDtypeStruct(block, bf),
            ),
            in_specs=[hbm] * 16,
            out_specs=(hbm, hbm),
            scratch_shapes=[
                VMEM((length, columns), bf),
                VMEM(block, bf),
                VMEM((top_count, 4 * TOK_DEV), jnp.int32),
                VMEM((top_count, 4 * TOK_DEV), f32),
                VMEM((1, width), f32),
                VMEM((heads, length), f32),
                VMEM((1, width), f32),
                VMEM((1, features), f32),
                VMEM((1, features), f32),
                VMEM((4,) + block, bf),
                VMEM((length, width), bf),
                VMEM((length, width), bf),
                VMEM((length, width), bf),
                VMEM((length, width), bf),
                VMEM(state_result_matrix.shape, bf),
                VMEM((features, hidden), bf),
                VMEM((features, hidden), bf),
                VMEM((hidden, features), bf),
                VMEM((4, capacity, hidden), bf),
                VMEM((4, experts, TOK_DEV), f32),
                VMEM((4, experts, TOK_DEV), f32),
                VMEM((planes, experts, TOK_DEV), f32),
                VMEM((planes,) + block, bf),
                VMEM((2, experts, TOK_DEV), f32),
                VMEM((2,) + block, bf),
                VMEM((n, 4) + chunk, bf),
                VMEM((n, 4) + chunk, bf),
                VMEM((2, n) + chunk, bf),
                VMEM((n,) + chunk, bf),
                VMEM((n,) + chunk, bf),
                VMEM((n,) + chunk, bf),
                VMEM((planes, group - 1) + chunk, bf),
                VMEM((group - 1,) + chunk, bf),
                VMEM((2, group - 1) + chunk, bf),
                VMEM(block, f32),
                VMEM((n * capacity, TOK_DEV), f32),
                VMEM((planes, TOK_DEV, TOK_DEV), bf),
                VMEM((planes, TOK_DEV, TOK_DEV), bf),
                VMEM((length, width), f32),
                VMEM((length, width), bf),
                VMEM((heads, HEAD, HEAD), f32),
                VMEM((heads, HEAD, HEAD), bf),
                VMEM((8, width), f32),
                VMEM((group, heads, HEAD, HEAD), bf),
                VMEM((group, 8, width), f32),
                VMEM((heads, HEAD, HEAD), bf),
                VMEM((heads, HEAD, HEAD), bf),
                VMEM((heads, HEAD, HEAD), f32),
                VMEM((heads, HEAD, HEAD), f32),
                VMEM((4, length, width), bf),
                DMA((16,)), DMA((PIECES,)), DMA((PIECES,)),
                DMA((2, planes, 2)), DMA((planes, 2)), DMA((2, planes)), DMA((planes,)),
                DMA((planes, group)), DMA((n,)), DMA((2, group)), DMA((2, n)),
                DMA((2, 3)), DMA((2, 3)), DMA((group,)), DMA((n,)),
                DMA((planes, group)), DMA((n,)),
            ]
            + [DMA((n,))] * 14
            + [DMA((group,))] * 4
            + [DMA, DMA]
            + [DMA((PIECES,))] * 6,
            compiler_params=pltpu.CompilerParams(
                collective_id=0, has_side_effects=True, vmem_limit_bytes=LIMIT * 2**20
            ),
        )(
            specialist_assignment.T,
            selected_specialist_share.T,
            retention_bound_margin[None, :],
            extra_fading_amount.T,
            state_result_scale[None, :],
            leading_scale_vector[None, :],
            trailing_scale_vector[None, :],
            second_slice_tokens.reshape((4,) + block),
            state_probe_logits,
            retention_logits,
            state_source_entries,
            state_result_switch_logits,
            state_result_matrix,
            specialist_switch_matrix[0],
            specialist_widen_matrix[0],
            specialist_contract_matrix[0],
        )
    )


def solution(mesh):
    return jax.shard_map(
        shards,
        mesh=mesh,
        in_specs=(
            P("ep", "tp"),
            P("ep", "tp"),
            P("ep", "tp"),
            P("ep", "tp"),
            P("tp"),
            P("ep", "tp"),
            P("tp"),
            P(None, "tp"),
            P("ep", None),
            P("ep", None),
            P("ep", None),
            P(),
            P(),
            P("ep", None, "tp"),
            P("ep", None, "tp"),
            P("ep", "tp", None),
        ),
        out_specs=(P("ep", "tp"), P(("ep", "tp"), None)),
        check_vma=False,
    )
```
